32 devices in a mesh: sp: 8 (over z, y), tp: 4 (over x, core).
Axes of the slice: x: 2, y: 2, z: 4, core: 2. Of those that a mesh axis runs over, the one named last changes fastest.
Arguments:
- queries: bfloat16 [1024, 2048], P('sp', 'tp'), may hold values from -6 to 6
- keys: bfloat16 [1024, 512], P('sp', 'tp'), may hold values from -6 to 6
- values: bfloat16 [1024, 512], P('sp', 'tp'), may hold values from -6 to 6
- query_gain: float32 [128], replicated, may hold values from 0.3 to 7
- key_norm_gain: float32 [128], replicated, may hold values from 0.3 to 7
- out_weight: bfloat16 [2048, 2048], P('tp'), may hold values from -0.25 to 0.25
- residual: bfloat16 [1024, 2048], P(('sp', 'tp')), may hold values from -6 to 6
- norm_gain: float32 [2048], replicated, may hold values from 0.1 to 1.9
- expert_gate: bfloat16 [8, 2048, 3072], P('sp', None, 'tp'), may hold values from -0.125 to 0.125
- expert_up: bfloat16 [8, 2048, 3072], P('sp', None, 'tp'), may hold values from -0.125 to 0.125
- expert_down: bfloat16 [8, 3072, 2048], P('sp', 'tp'), may hold values from -0.109375 to 0.109375
- routes: int32 [1024, 2], P(('sp', 'tp')), may hold values from 0 to 7, all different within a row; in each aligned block of 32 rows (0 to 31, 32 to 63, ...) at most 16 rows name the same one
- route_weight: float32 [1024, 2], P(('sp', 'tp')), may hold values from 0.25 to 1
Outputs:
- mixed: bfloat16 [1024, 2048], P(('sp', 'tp'))
The draws below stay inside these ranges and needn't reach their ends.
Inputs may be any that keep to these rules, and one draw needn't show every extreme that they name: The two experts of a token differ. In each aligned block of 32 tokens (the tokens of one device), no expert is named by more than 16 routes, and in some block one expert is named by exactly 16.
All inputs are finite; a program needn't handle non-finite values.
Results may differ from the reference program's by a relative error of at most 0.013.
The reference program's roundings to bfloat16 on the way count: a program that leaves them out, or rounds other values in their place, can miss the bound.
Values may be sent and summed in bfloat16 or wider, within the bound.
No kernel may reach another device: no remote copies, remote signals or barrier semaphores. Data moves between devices by JAX's collectives and lax.ppermute only.
A program may use at most 64 MiB of HBM per device.

```python
import math
import jax
import jax.numpy as jnp
import numpy as np
from jax import lax

D = 2048
QUERY_HEAD_COUNT = 16
KEY_VALUE_HEADS = 4
HEAD_SIZE = 128
FE = 3072
TOP = 2
GRID_W = 64
TOK_DEV = 128
SEQUENCE_TOKENS = 1024
EXPERTS = 8
CAP = 16
N_SP = 8
N_TP = 4


def shared_gain(key, salt_value):
    uniform_unit = jax.random.uniform(jax.random.fold_in(key, salt_value), (HEAD_SIZE,), jnp.float32)
    return jnp.exp(jnp.log(1.2) + uniform_unit * (jnp.log(2.5) - jnp.log(1.2)))


def draw_query_gain(key, part):
    return shared_gain(key, 102)


def draw_key_norm_gain(key, part):
    return shared_gain(key, 103)


def build_keys(key):
    base_sample = jnp.clip(jax.random.normal(jax.random.fold_in(key, 104), (SEQUENCE_TOKENS, KEY_VALUE_HEADS * HEAD_SIZE), jnp.float32), -6.0, 6.0)
    return base_sample


def draw_keys(key, part):
    return build_keys(key).astype(jnp.bfloat16)


def draw_queries(key, part):
    base_sample = jnp.clip(jax.random.normal(jax.random.fold_in(key, 105), (SEQUENCE_TOKENS, QUERY_HEAD_COUNT * HEAD_SIZE), jnp.float32), -6.0, 6.0)
    return base_sample.astype(jnp.bfloat16)


def levels(stream_key, dims, cuts, smallest, top_value):
    def one(position, shards_of):
        steps = jax.random.uniform(jax.random.fold_in(jax.random.fold_in(stream_key, 6), position), (shards_of,), jnp.float32, smallest / len(cuts), top_value / len(cuts))
        return jnp.repeat(jnp.exp(steps), dims[position] // shards_of).reshape((-1,) + (1,) * (len(dims) - position - 1))

    level = one(*cuts[0])
    for cut in cuts[1:]:
        level = level * one(*cut)
    return level


def assign_block(key, own, number, rows, amount, top, reach, skew):
    ranking = jax.random.permutation(key, amount)
    crowded, usual = portions_of(amount, rows * top, reach, skew, True), portions_of(amount, rows * top, reach, skew, False)
    places = jnp.arange(amount)

    def named(sizes, rotation):
        used = int((sizes > 0).sum())
        fixed = max(1, used // 4)
        shifted = fixed + (places - fixed + rotation * (used - fixed)) % max(1, amount - fixed)
        return jnp.zeros((amount,), jnp.int32).at[ranking[jnp.where(places < fixed, places, shifted)]].set(jnp.asarray(sizes, jnp.int32))

    sizes = jnp.where(number % 4 == 0, named(crowded, number // 4), named(usual, number - number // 4 - 1))
    mixed = jax.random.permutation(jax.random.fold_in(own, 3), amount)
    donor, sink = mixed[0:amount // 2 * 2:2], mixed[1:amount // 2 * 2:2]
    margin = jnp.minimum(sizes[donor] - 1, reach - sizes[sink]) // 2
    margin = jnp.where((donor == ranking[0]) | (sink == ranking[0]) | (sizes[sink] == 0), 0, jnp.maximum(margin, 0))
    shifted = jax.random.randint(jax.random.fold_in(own, 4), (amount // 2,), 0, 1 << 20) % (margin + 1)
    sizes = sizes.at[donor].add(-shifted).at[sink].add(shifted)
    labels = jnp.searchsorted(jnp.cumsum(sizes), jnp.arange(rows * top), side="right").astype(jnp.int32)
    grid = labels.reshape(top, rows).T
    grid = grid[jax.random.permutation(jax.random.fold_in(own, 1), rows)]
    rotation = jax.random.randint(jax.random.fold_in(own, 2), (rows, 1), 0, top)
    return jnp.take_along_axis(grid, (jnp.arange(top)[None, :] + rotation) % top, axis=1)


def portions_of(count, total, bound, skew, full):
    portions = [(1 << 20) // math.isqrt(standing ** skew) + 1 for standing in range(1, count + 1)]
    largest = bound if full else min(bound, max(-(-total // count), total * portions[0] // sum(portions)))
    least = 1 if total - largest >= count - 1 else 0
    holding, spare = [largest] + [least] * (count - 1), total - largest - least * (count - 1)
    while spare > 0:
        free = [i for i in range(1, count) if holding[i] < largest] or [i for i in range(1, count) if holding[i] < bound]
        whole, budget = sum([portions[i] for i in free]), spare
        for i in free:
            extra = min(bound - holding[i], max(1, budget * portions[i] // whole), spare)
            holding[i] = holding[i] + extra
            spare = spare - extra
    return np.array(holding)


def bell_draw(rng, shape, width, reach, split=(), kind=jnp.bfloat16):
    entries = jax.random.normal(rng, shape, jnp.float32) * width
    if len(split) > 0:
        entries = levels(rng, shape, split, -0.22, 0.18) * entries
    return jnp.clip(entries, min=-reach, max=reach).astype(kind)


def setup_inputs(seed: int = 0) -> dict:
    streams_of = jax.random.split(jax.random.key(seed), 14)
    queries = draw_queries(jax.random.fold_in(streams_of[13], 71), 0)
    keys = draw_keys(jax.random.fold_in(streams_of[13], 71), 0)
    values = bell_draw(streams_of[2], (SEQUENCE_TOKENS, KEY_VALUE_HEADS * HEAD_SIZE), 1.0, 6.0, ((0, 8), (1, 4)))
    query_gain = draw_query_gain(jax.random.fold_in(streams_of[13], 71), 0)
    key_norm_gain = draw_key_norm_gain(jax.random.fold_in(streams_of[13], 71), 0)
    out_weight = bell_draw(streams_of[5], (QUERY_HEAD_COUNT * HEAD_SIZE, D), (QUERY_HEAD_COUNT * HEAD_SIZE // 4) ** -0.5, 0.25, ((0, 4),))
    residual = bell_draw(streams_of[6], (SEQUENCE_TOKENS, D), 1.0, 6.0, ((0, 32),))
    norm_gain = jnp.clip(1.0 + 0.18 * jax.random.normal(streams_of[7], (D,), jnp.float32), 0.1, 1.9)
    expert_gate = bell_draw(streams_of[8], (EXPERTS, D, FE), D ** -0.5, 0.125, ((0, 8), (2, 4)))
    expert_up = bell_draw(streams_of[9], (EXPERTS, D, FE), D ** -0.5, 0.125, ((0, 8), (2, 4)))
    expert_down = bell_draw(streams_of[10], (EXPERTS, FE, D), FE ** -0.5, 0.109375, ((0, 8), (1, 4)))
    routes_keys = jax.random.split(jax.random.fold_in(streams_of[11], 1), SEQUENCE_TOKENS // (TOK_DEV // N_TP))
    routes_turns = jax.random.permutation(jax.random.fold_in(streams_of[11], 3), SEQUENCE_TOKENS // (TOK_DEV // N_TP))
    routes = jax.vmap(lambda own, number: assign_block(jax.random.fold_in(streams_of[11], 2), own, number, TOK_DEV // N_TP, EXPERTS, TOP, CAP, 2))(routes_keys, routes_turns).reshape((SEQUENCE_TOKENS, TOP))
    route_weight = jnp.clip(0.25 + 0.75 * jax.random.uniform(streams_of[12], (SEQUENCE_TOKENS, TOP), jnp.float32) ** levels(streams_of[12], (SEQUENCE_TOKENS, TOP), ((0, 32),), -0.2, 0.2), 0.25, 1.0)
    return {"queries": queries, "keys": keys, "values": values, "query_gain": query_gain, "key_norm_gain": key_norm_gain, "out_weight": out_weight, "residual": residual, "norm_gain": norm_gain, "expert_gate": expert_gate, "expert_up": expert_up, "expert_down": expert_down, "routes": routes, "route_weight": route_weight}


norm_eps = 1e-06
theta_base = 10000.0

def round_to_half(array):
    return lax.optimization_barrier(array.astype(jnp.bfloat16)).astype(jnp.float32)

def head_normalize(packed, gain, heads):
    heads_float = packed.astype(jnp.float32).reshape(packed.shape[0], heads, HEAD_SIZE)
    scaled = heads_float * lax.rsqrt(lax.optimization_barrier(jnp.mean(heads_float * heads_float, axis=-1, keepdims=True)) + norm_eps)
    return scaled * gain.astype(jnp.float32)

def rotary_tables(positions):
    freq_count = HEAD_SIZE // 4
    grid_row = (positions // GRID_W).astype(jnp.float32)
    grid_col = (positions % GRID_W).astype(jnp.float32)
    inverse = theta_base ** (-jnp.arange(freq_count, dtype=jnp.float32) * 2.0 / (HEAD_SIZE // 2))
    by_row = grid_row[:, None] * inverse
    by_col = grid_col[:, None] * inverse
    angles = jnp.concatenate([by_row, by_row, by_col, by_col], axis=-1)
    return (jnp.cos(angles), jnp.sin(angles))

def apply_rotation(heads_float, cosine_table, sine_values):
    freq_count = HEAD_SIZE // 4
    split_head = heads_float.reshape(heads_float.shape[:-1] + (2, 2, freq_count))
    turned = jnp.stack([-split_head[..., 1, :], split_head[..., 0, :]], axis=-2).reshape(heads_float.shape)
    return heads_float * cosine_table[:, None, :] + turned * sine_values[:, None, :]

def reference(queries, keys, values, query_gain, key_norm_gain, out_weight, residual, norm_gain, expert_gate, expert_up, expert_down, routes, route_weight):
    score_scale = 1.0 / math.sqrt(HEAD_SIZE)
    group_members = QUERY_HEAD_COUNT // KEY_VALUE_HEADS
    positions = jnp.arange(SEQUENCE_TOKENS, dtype=jnp.int32)
    cosine_table, sine_values = rotary_tables(positions)
    rotated_queries = apply_rotation(head_normalize(queries, query_gain, QUERY_HEAD_COUNT), cosine_table, sine_values).astype(jnp.bfloat16)
    rotated_keys = round_to_half(apply_rotation(head_normalize(keys, key_norm_gain, KEY_VALUE_HEADS), cosine_table, sine_values))
    value_wide_float = values.reshape(SEQUENCE_TOKENS, KEY_VALUE_HEADS, HEAD_SIZE).astype(jnp.float32)
    query_tile_rows = math.gcd(SEQUENCE_TOKENS, 128)
    block_list = rotated_queries.reshape(SEQUENCE_TOKENS // query_tile_rows, query_tile_rows, KEY_VALUE_HEADS, group_members, HEAD_SIZE)

    def attend(query_part):
        scores = jnp.einsum('qkgd,skd->kgqs', query_part.astype(jnp.float32), rotated_keys) * score_scale
        row_max = lax.optimization_barrier(jnp.max(scores, axis=-1, keepdims=True))
        weights = jnp.exp(scores - row_max)
        norm_sum = lax.optimization_barrier(jnp.sum(weights, axis=-1))
        value_sum = jnp.einsum('kgqs,skd->kgqd', round_to_half(weights), value_wide_float)
        result = value_sum / norm_sum[..., None]
        return result.transpose(2, 0, 1, 3).reshape(query_tile_rows, QUERY_HEAD_COUNT * HEAD_SIZE).astype(jnp.bfloat16)
    attention = lax.map(attend, block_list).reshape(SEQUENCE_TOKENS, QUERY_HEAD_COUNT * HEAD_SIZE)
    projected = jnp.dot(attention, out_weight, preferred_element_type=jnp.float32)
    hidden_state = residual.astype(jnp.float32) + projected
    normed = (hidden_state * lax.rsqrt(lax.optimization_barrier(jnp.mean(hidden_state * hidden_state, axis=-1, keepdims=True)) + norm_eps) * norm_gain.astype(jnp.float32)).astype(jnp.bfloat16)
    slots_most = N_SP * N_TP * CAP
    flat_routes = routes.reshape(-1)
    flat_weight = route_weight.reshape(-1).astype(jnp.float32)
    piece_width = FE // N_TP

    def expert_step(total, inputs):
        expert, gate_weight, up_weight, down_weight = inputs
        chosen = flat_routes == expert
        route_index = jnp.nonzero(chosen, size=slots_most, fill_value=0)[0].astype(jnp.int32)
        live_mask = (jnp.arange(slots_most, dtype=jnp.int32) < jnp.sum(chosen.astype(jnp.int32))).astype(jnp.float32)
        owner_row = route_index // TOP
        rows_in = normed[owner_row]
        gate_proj = jnp.dot(rows_in, gate_weight, preferred_element_type=jnp.float32)
        up_proj = jnp.dot(rows_in, up_weight, preferred_element_type=jnp.float32)
        hidden_act = (jax.nn.silu(gate_proj) * up_proj).astype(jnp.bfloat16)
        summed = jnp.zeros((slots_most, D), jnp.float32)
        for quarter in range(N_TP):
            down_part = jnp.dot(hidden_act[:, quarter * piece_width:(quarter + 1) * piece_width], down_weight[quarter * piece_width:(quarter + 1) * piece_width], preferred_element_type=jnp.float32)
            summed = summed + round_to_half(down_part)
        output = round_to_half(summed)
        total = total.at[owner_row].add((flat_weight[route_index] * live_mask)[:, None] * output)
        return (total, None)
    moe_sum, _ = lax.scan(expert_step, jnp.zeros((SEQUENCE_TOKENS, D), jnp.float32), (jnp.arange(EXPERTS, dtype=jnp.int32), expert_gate, expert_up, expert_down))
    return (hidden_state + moe_sum).astype(jnp.bfloat16)
```

```python
import math

import jax
import jax.numpy as jnp
from jax import lax
from jax.experimental import pallas as pl
from jax.experimental.pallas import tpu as pltpu
from jax.sharding import PartitionSpec as P

HEAD_SIZE = 128
GRID_W = 64
norm_eps = 1e-06
theta_base = 10000.0


F32 = jnp.float32
BF16 = jnp.bfloat16
VM = pl.BlockSpec(memory_space=pltpu.VMEM)
SM = pl.BlockSpec(memory_space=pltpu.SMEM)
ANY = pl.BlockSpec(memory_space=pl.ANY)


def params(mib):
    return pltpu.CompilerParams(vmem_limit_bytes=mib * 1024 * 1024)


def swap(x, axis, k):
    n = lax.axis_size(axis)
    return lax.ppermute(x, axis, [(i, i ^ k) for i in range(n)])


def rotate_norm(x, gain, cosine, sine):
    ms = jnp.mean(x * x, axis=-1, keepdims=True)
    v = x * lax.rsqrt(ms + norm_eps) * gain
    lane = lax.broadcasted_iota(jnp.int32, v.shape, 1)
    quarter = HEAD_SIZE // 4
    turned = jnp.where(
        (lane & (2 * quarter - 1)) < quarter,
        -pltpu.roll(v, HEAD_SIZE - quarter, 1),
        pltpu.roll(v, quarter, 1),
    )
    return v * cosine + turned * sine


def key_kernel(sp_ref, inv_ref, gain_ref, k_ref, v_ref, kv_ref, cos_ref, sin_ref):
    rows = k_ref.shape[0]
    kw = k_ref.shape[1]
    pos = sp_ref[0] * rows + lax.broadcasted_iota(jnp.int32, (rows, HEAD_SIZE), 0)
    lane = lax.broadcasted_iota(jnp.int32, (rows, HEAD_SIZE), 1)
    shift = GRID_W.bit_length() - 1
    coord = jnp.where(lane < HEAD_SIZE // 2, pos >> shift, pos & (GRID_W - 1)).astype(F32)
    angles = coord * inv_ref[...]
    cosine = jnp.cos(angles)
    sine = jnp.sin(angles)
    cos_ref[...] = cosine
    sin_ref[...] = sine
    for h in range(kw // HEAD_SIZE):
        cols = slice(h * HEAD_SIZE, (h + 1) * HEAD_SIZE)
        kv_ref[:, cols] = rotate_norm(
            k_ref[:, cols].astype(F32), gain_ref[...], cosine, sine
        ).astype(BF16)
    kv_ref[:, kw:] = v_ref[...]


def query_kernel(gain_ref, cos_ref, sin_ref, q_ref, o_ref):
    rows = q_ref.shape[0]
    for h in range(q_ref.shape[1] // HEAD_SIZE):
        o_ref[h * rows : (h + 1) * rows, :] = rotate_norm(
            q_ref[:, h * HEAD_SIZE : (h + 1) * HEAD_SIZE].astype(F32),
            gain_ref[...],
            cos_ref[...],
            sin_ref[...],
        ).astype(BF16)


def attention_kernel(npieces, tp_size, tp_ref, q_ref, *rest):
    kv_refs = rest[:npieces]
    w_hbm, keep_ref, send_ref, s_scr, att_scr, w_scr, sem = rest[npieces:]
    copy = pltpu.make_async_copy(w_hbm, w_scr, sem)
    copy.start()
    kw = kv_refs[0].shape[1] // 2
    key_heads = kw // HEAD_SIZE
    rows = att_scr.shape[0]
    heads = q_ref.shape[0] // rows
    members = heads // key_heads
    piece = kv_refs[0].shape[0]
    scale = math.log2(math.e) / math.sqrt(HEAD_SIZE)
    pair = 2 if npieces % 2 == 0 else 1
    span = pair * piece

    def load(i, col):
        return jnp.concatenate(
            [kv_refs[i * pair + j][:, col : col + HEAD_SIZE] for j in range(pair)], axis=0
        )

    for h in range(heads):
        kc = (h // members) * HEAD_SIZE
        q = q_ref[h * rows : (h + 1) * rows, :]
        top = None
        for i in range(npieces // pair):
            s = lax.dot_general(
                q, load(i, kc), (((1,), (1,)), ((), ())), preferred_element_type=F32
            )
            s_scr[:, i * span : (i + 1) * span] = s
            top = s if top is None else jnp.maximum(top, s)
        m = jnp.max(top, axis=-1, keepdims=True) * scale
        total = None
        acc = None
        for i in range(npieces // pair):
            p = jnp.exp2(s_scr[:, i * span : (i + 1) * span] * scale - m)
            total = p if total is None else total + p
            o = jnp.dot(p.astype(BF16), load(i, kw + kc), preferred_element_type=F32)
            acc = o if acc is None else acc + o
        norm = jnp.sum(total, axis=-1, keepdims=True)
        att_scr[:, h * HEAD_SIZE : (h + 1) * HEAD_SIZE] = (acc / norm).astype(BF16)
    copy.wait()
    t = tp_ref[0]
    block = rows // tp_size
    for half, ref in ((0, keep_ref), (1, send_ref)):
        lhs = jnp.concatenate(
            [
                att_scr[pl.ds(pl.multiple_of((t ^ j) * block, block), block), :]
                for j in range(half, tp_size, 2)
            ],
            axis=0,
        )
        ref[...] = jnp.dot(lhs, w_scr[...], preferred_element_type=F32).astype(ref.dtype)


def dispatch_kernel(cap, slot_ref, gain_ref, res_ref, keep_ref, r1_ref, r2_ref, hid_ref, *outs):
    rows = res_ref.shape[0]
    hidden = (
        res_ref[...].astype(F32)
        + keep_ref[:rows, :]
        + r1_ref[:rows, :].astype(F32)
        + r2_ref[...].astype(F32)
    )
    hid_ref[...] = hidden
    ms = jnp.mean(hidden * hidden, axis=-1, keepdims=True)
    normed = (hidden * lax.rsqrt(ms + norm_eps) * gain_ref[...]).astype(BF16)

    def pick(first, count):
        slot = first + lax.broadcasted_iota(jnp.int32, (count, rows), 0)
        hit = slot == slot_ref[0:1, :]
        for j in range(1, slot_ref.shape[0]):
            hit = hit | (slot == slot_ref[j : j + 1, :])
        return jnp.dot(hit.astype(BF16), normed, preferred_element_type=F32).astype(BF16)

    if cap % 16 == 0:
        picked = pick(0, cap * len(outs))
        for k, ref in enumerate(outs):
            ref[...] = picked[k * cap : (k + 1) * cap, :]
    else:
        for k, ref in enumerate(outs):
            ref[...] = pick(k * cap, cap)


def expert_kernel(nrow, fc, *refs):
    x_refs = refs[:nrow]
    g_hbm, u_hbm, d_hbm, keep_ref, send_ref, g_scr, u_scr, d_scr, acc, sems = refs[nrow:]
    chunks = g_scr.shape[0]
    copies = []
    for f in range(chunks):
        cs = (
            pltpu.make_async_copy(g_hbm.at[0, :, pl.ds(f * fc, fc)], g_scr.at[f], sems.at[0, f]),
            pltpu.make_async_copy(u_hbm.at[0, :, pl.ds(f * fc, fc)], u_scr.at[f], sems.at[1, f]),
            pltpu.make_async_copy(d_hbm.at[0, pl.ds(f * fc, fc), :], d_scr.at[f], sems.at[2, f]),
        )
        for c in cs:
            c.start()
        copies.append(cs)
    x = jnp.concatenate([r[...] for r in x_refs], axis=0)
    for f in range(chunks):
        copies[f][0].wait()
        copies[f][1].wait()
        gate = jnp.dot(x, g_scr[f], preferred_element_type=F32)
        up = jnp.dot(x, u_scr[f], preferred_element_type=F32)
        act = (gate / (1.0 + jnp.exp(-gate)) * up).astype(BF16)
        copies[f][2].wait()
        part = jnp.dot(act, d_scr[f], preferred_element_type=F32)
        if chunks == 1:
            total = part
        elif f == 0:
            acc[...] = part
            total = None
        elif f < chunks - 1:
            acc[...] += part
            total = None
        else:
            total = acc[...] + part
    half = total.shape[0] // 2
    keep_ref[...] = total[:half].astype(BF16)
    send_ref[...] = total[half:].astype(BF16)


def settle_kernel(keep_ref, r1_ref, r2_ref, *outs):
    rows = r2_ref.shape[0]
    each = rows // len(outs)
    total = (
        keep_ref[:rows, :].astype(F32) + r1_ref[:rows, :].astype(F32) + r2_ref[...].astype(F32)
    ).astype(BF16)
    for k, ref in enumerate(outs):
        ref[...] = total[k * each : (k + 1) * each, :]


def combine_kernel(slot_ref, weight_ref, hid_ref, *refs):
    parts, out_ref = refs[:-1], refs[-1]
    back = jnp.concatenate([r[...] for r in parts], axis=0)
    rows = hid_ref.shape[0]
    slot = lax.broadcasted_iota(jnp.int32, (rows, back.shape[0]), 1)
    total = hid_ref[...]
    for j in range(slot_ref.shape[1]):
        hit = (slot == slot_ref[:, j : j + 1]).astype(BF16)
        total += weight_ref[:, j : j + 1] * jnp.dot(hit, back, preferred_element_type=F32)
    out_ref[...] = total.astype(out_ref.dtype)


def shaped(shape, dtype):
    return jax.ShapeDtypeStruct(shape, dtype)


def on_device(
    queries, keys, values, query_gain, key_norm_gain, out_weight, residual, norm_gain,
    expert_gate, expert_up, expert_down, routes, route_weight,
):
    sp_size, tp_size = lax.axis_size("sp"), lax.axis_size("tp")
    sp, tp = lax.axis_index("sp"), lax.axis_index("tp")
    rows = queries.shape[0]
    qw, kw = queries.shape[1], keys.shape[1]
    heads = qw // HEAD_SIZE
    own, width = residual.shape
    route_top = routes.shape[1]
    experts = sp_size * expert_gate.shape[0]
    cap = 2 * max(1, route_top * rows // (tp_size * experts))
    sp1, tp1 = sp.astype(jnp.int32).reshape(1), tp.astype(jnp.int32).reshape(1)
    freq = HEAD_SIZE // 4
    inverse = theta_base ** (
        -(jnp.arange(HEAD_SIZE, dtype=jnp.int32) % freq).astype(F32) * 2.0 / (HEAD_SIZE // 2)
    )
    inverse = inverse.reshape(1, HEAD_SIZE)

    kv, cosine, sine = pl.pallas_call(
        key_kernel,
        out_shape=(
            shaped((rows, 2 * kw), BF16),
            shaped((rows, HEAD_SIZE), F32),
            shaped((rows, HEAD_SIZE), F32),
        ),
        in_specs=[SM, VM, VM, VM, VM],
        out_specs=(VM, VM, VM),
        compiler_params=params(4),
        name="key_prep",
    )(sp1, inverse, key_norm_gain.reshape(1, -1), keys, values)

    half = sp_size // 2
    far = swap(kv, "sp", half)
    near = [swap(kv, "sp", k) for k in range(1, half)]
    far_rest = [swap(far, "sp", k) for k in range(1, half)]
    pieces = [kv] + near + [far] + far_rest
    if len(pieces) > 8:
        each = len(pieces) // 8
        pieces = [jnp.concatenate(pieces[i * each : (i + 1) * each], axis=0) for i in range(8)]

    q = pl.pallas_call(
        query_kernel,
        out_shape=shaped((heads * rows, HEAD_SIZE), BF16),
        in_specs=[VM] * 4,
        out_specs=VM,
        compiler_params=params(4),
        name="query_prep",
    )(query_gain.reshape(1, -1), cosine, sine, queries)

    flat = routes.reshape(-1)
    onehot = (flat[:, None] == jnp.arange(experts, dtype=jnp.int32)[None, :]).astype(jnp.int32)
    earlier = jnp.cumsum(onehot, axis=0) - onehot
    rank = jnp.sum(earlier * onehot, axis=1)
    slot = ((flat ^ sp.astype(jnp.int32)) * cap + rank).reshape(own, route_top)
    slot_t = slot.T

    keys_all = sum(p.shape[0] for p in pieces)
    keep, send = pl.pallas_call(
        lambda *a: attention_kernel(len(pieces), tp_size, *a),
        out_shape=(shaped((rows // 2, width), F32), shaped((rows // 2, width), BF16)),
        in_specs=[SM, VM] + [VM] * len(pieces) + [ANY],
        out_specs=(VM, VM),
        scratch_shapes=[
            pltpu.VMEM((rows, keys_all), F32),
            pltpu.VMEM((rows, qw), BF16),
            pltpu.VMEM(out_weight.shape, BF16),
            pltpu.SemaphoreType.DMA,
        ],
        compiler_params=params(24),
        name="attend",
    )(tp1, q, *pieces, out_weight)

    r1 = swap(send, "tp", 1)
    pair = (keep[own:] + r1[own:].astype(F32)).astype(BF16)
    r2 = swap(pair, "tp", 2)

    picked = pl.pallas_call(
        lambda *a: dispatch_kernel(cap, *a),
        out_shape=[shaped((own, width), F32)] + [shaped((cap, width), BF16)] * sp_size,
        in_specs=[VM] * 6,
        out_specs=[VM] * (1 + sp_size),
        compiler_params=params(8),
        name="dispatch",
    )(slot_t, norm_gain.reshape(1, -1), residual, keep, r1, r2)
    hidden, mail = picked[0], picked[1:]

    inbox = [mail[0]] + [swap(mail[k], "sp", k) for k in range(1, sp_size)]
    fe = expert_gate.shape[2]
    fc = 256 if fe % 256 == 0 else fe
    returned = []
    for c in range(2):
        mine = jnp.concatenate(inbox[c * half : (c + 1) * half], axis=0)
        core = swap(mine, "tp", 1)
        cross = swap(mine, "tp", 2)
        both = swap(cross, "tp", 1)
        n = mine.shape[0]
        keep_e, send_e = pl.pallas_call(
            lambda *a: expert_kernel(4, fc, *a),
            out_shape=(shaped((2 * n, width), BF16), shaped((2 * n, width), BF16)),
            in_specs=[VM] * 4 + [ANY] * 3,
            out_specs=(VM, VM),
            scratch_shapes=[
                pltpu.VMEM((fe // fc, width, fc), BF16),
                pltpu.VMEM((fe // fc, width, fc), BF16),
                pltpu.VMEM((fe // fc, fc, width), BF16),
                pltpu.VMEM((4 * n, width), F32),
                pltpu.SemaphoreType.DMA((3, fe // fc)),
            ],
            compiler_params=params(32),
            name="experts",
        )(mine, cross, core, both, expert_gate, expert_up, expert_down)
        e1 = swap(send_e, "tp", 1)
        pair_e = (keep_e[n:].astype(F32) + e1[n:].astype(F32)).astype(BF16)
        e2 = swap(pair_e, "tp", 2)
        settled = pl.pallas_call(
            settle_kernel,
            out_shape=[shaped((cap, width), BF16)] * half,
            in_specs=[VM] * 3,
            out_specs=[VM] * half,
            compiler_params=params(8),
            name="settle",
        )(keep_e, e1, e2)
        for k in range(half):
            peer = c * half + k
            returned.append(swap(settled[k], "sp", peer) if peer else settled[k])

    return pl.pallas_call(
        combine_kernel,
        out_shape=shaped((own, width), BF16),
        in_specs=[VM] * (3 + sp_size),
        out_specs=VM,
        compiler_params=params(8),
        name="combine",
    )(slot, route_weight, hidden, *returned)


def solution(mesh):
    placed = (
        P("sp", "tp"),
        P("sp", "tp"),
        P("sp", "tp"),
        P(),
        P(),
        P("tp", None),
        P(("sp", "tp"), None),
        P(),
        P("sp", None, "tp"),
        P("sp", None, "tp"),
        P("sp", "tp", None),
        P(("sp", "tp"), None),
        P(("sp", "tp"), None),
    )
    return jax.shard_map(
        on_device, mesh=mesh, in_specs=placed, out_specs=P(("sp", "tp"), None), check_vma=False
    )
```

```python
import math

import jax
import jax.numpy as jnp
from jax import lax
from jax.experimental import pallas as pl
from jax.experimental.pallas import tpu as pltpu
from jax.sharding import PartitionSpec as P

HEAD_SIZE = 128
GRID_W = 64
norm_eps = 1e-06
theta_base = 10000.0


F32 = jnp.float32
BF16 = jnp.bfloat16
VM = pl.BlockSpec(memory_space=pltpu.VMEM)
SM = pl.BlockSpec(memory_space=pltpu.SMEM)
ANY = pl.BlockSpec(memory_space=pl.ANY)


def params(mib):
    return pltpu.CompilerParams(vmem_limit_bytes=mib * 1024 * 1024)


def swap(x, axis, k):
    n = lax.axis_size(axis)
    return lax.ppermute(x, axis, [(i, i ^ k) for i in range(n)])


def rotate_norm(x, gain, cosine, sine):
    ms = jnp.mean(x * x, axis=-1, keepdims=True)
    v = x * lax.rsqrt(ms + norm_eps) * gain
    lane = lax.broadcasted_iota(jnp.int32, v.shape, 1)
    quarter = HEAD_SIZE // 4
    turned = jnp.where(
        (lane & (2 * quarter - 1)) < quarter,
        -pltpu.roll(v, HEAD_SIZE - quarter, 1),
        pltpu.roll(v, quarter, 1),
    )
    return v * cosine + turned * sine


def fetch(pairs, sem):
    copies = [pltpu.make_async_copy(src, dst, sem.at[i]) for i, (src, dst) in enumerate(pairs)]
    for c in copies:
        c.start()
    return copies


def key_kernel(sp_ref, gain_ref, k_ref, v_ref, kv_ref, cos_ref, sin_ref, k_scr, g_scr, sem):
    kw = k_scr.shape[1]
    copies = fetch(
        ((k_ref, k_scr), (gain_ref, g_scr), (v_ref, kv_ref.at[:, pl.ds(kw, kw)])), sem
    )
    rows = k_scr.shape[0]
    pos = sp_ref[0] * rows + lax.broadcasted_iota(jnp.int32, (rows, HEAD_SIZE), 0)
    lane = lax.broadcasted_iota(jnp.int32, (rows, HEAD_SIZE), 1)
    shift = GRID_W.bit_length() - 1
    coord = jnp.where(lane < HEAD_SIZE // 2, pos >> shift, pos & (GRID_W - 1)).astype(F32)
    freq = (lane & (HEAD_SIZE // 4 - 1)).astype(F32)
    angles = coord * jnp.exp(freq * (-2.0 * math.log(theta_base) / (HEAD_SIZE // 2)))
    cosine = jnp.cos(angles)
    sine = jnp.sin(angles)
    cos_ref[...] = cosine
    sin_ref[...] = sine
    copies[0].wait()
    copies[1].wait()
    for h in range(kw // HEAD_SIZE):
        cols = slice(h * HEAD_SIZE, (h + 1) * HEAD_SIZE)
        kv_ref[:, cols] = rotate_norm(
            k_scr[:, cols].astype(F32), g_scr[...], cosine, sine
        ).astype(BF16)
    copies[2].wait()


def attention_kernel(npieces, tp_size, tp_ref, cos_ref, sin_ref, gain_ref, q_ref, w_ref, *rest):
    kv_refs = rest[:npieces]
    keep_ref, send_ref, s_scr, att_scr, q_scr, g_scr, sem = rest[npieces:]
    copies = fetch(((q_ref, q_scr), (gain_ref, g_scr)), sem)
    kw = kv_refs[0].shape[1] // 2
    key_heads = kw // HEAD_SIZE
    rows = att_scr.shape[0]
    heads = q_scr.shape[1] // HEAD_SIZE
    members = heads // key_heads
    piece = kv_refs[0].shape[0]
    scale = math.log2(math.e) / math.sqrt(HEAD_SIZE)
    pair = 2 if npieces % 2 == 0 else 1
    span = pair * piece

    def load(i, col):
        return jnp.concatenate(
            [kv_refs[i * pair + j][:, col : col + HEAD_SIZE] for j in range(pair)], axis=0
        )

    for c in copies:
        c.wait()
    for h in range(heads):
        kc = (h // members) * HEAD_SIZE
        q = rotate_norm(
            q_scr[:, h * HEAD_SIZE : (h + 1) * HEAD_SIZE].astype(F32),
            g_scr[...],
            cos_ref[...],
            sin_ref[...],
        ).astype(BF16)
        top = None
        for i in range(npieces // pair):
            s = lax.dot_general(
                q, load(i, kc), (((1,), (1,)), ((), ())), preferred_element_type=F32
            )
            s_scr[:, i * span : (i + 1) * span] = s
            top = s if top is None else jnp.maximum(top, s)
        m = jnp.max(top, axis=-1, keepdims=True) * scale
        total = None
        acc = None
        for i in range(npieces // pair):
            p = jnp.exp2(s_scr[:, i * span : (i + 1) * span] * scale - m)
            total = p if total is None else total + p
            o = jnp.dot(p.astype(BF16), load(i, kw + kc), preferred_element_type=F32)
            acc = o if acc is None else acc + o
        norm = jnp.sum(total, axis=-1, keepdims=True)
        att_scr[:, h * HEAD_SIZE : (h + 1) * HEAD_SIZE] = (acc / norm).astype(BF16)
    t = tp_ref[0]
    block = rows // tp_size
    for half, ref in ((0, keep_ref), (1, send_ref)):
        lhs = jnp.concatenate(
            [
                att_scr[pl.ds(pl.multiple_of((t ^ j) * block, block), block), :]
                for j in range(half, tp_size, 2)
            ],
            axis=0,
        )
        ref[...] = jnp.dot(lhs, w_ref[...], preferred_element_type=F32).astype(ref.dtype)


def pair_kernel(keep_ref, got_ref, out_ref):
    rows = out_ref.shape[0]
    out_ref[...] = (
        keep_ref[rows:, :].astype(F32) + got_ref[rows:, :].astype(F32)
    ).astype(out_ref.dtype)


def base_kernel(
    experts, cap, sp_ref, dep_ref, routes_ref, res_ref, gain_ref, keep_ref, r1_ref,
    slot_ref, base_ref, gain_out, routes_scr, res_scr, sem,
):
    copies = fetch(((routes_ref, routes_scr), (res_ref, res_scr), (gain_ref, gain_out)), sem)
    top, rows = slot_ref.shape
    expert = lax.broadcasted_iota(jnp.int32, (experts, rows), 0)
    before = lax.broadcasted_iota(jnp.int32, (rows, rows), 0) < lax.broadcasted_iota(
        jnp.int32, (rows, rows), 1
    )
    copies[0].wait()
    marks = [(expert == routes_scr[j : j + 1, :]).astype(F32) for j in range(top)]
    earlier = jnp.dot(
        sum(marks).astype(BF16), before.astype(BF16), preferred_element_type=F32
    )
    for j in range(top):
        rank = jnp.sum(earlier * marks[j], axis=0, keepdims=True).astype(jnp.int32)
        slot_ref[j : j + 1, :] = (routes_scr[j : j + 1, :] ^ sp_ref[0]) * cap + rank
    copies[1].wait()
    base_ref[...] = (
        res_scr[...].astype(F32) + keep_ref[:rows, :].astype(F32) + r1_ref[:rows, :].astype(F32)
    )
    copies[2].wait()


def dispatch_kernel(cap, slot_ref, gain_ref, base_ref, r2_ref, hid_ref, *outs):
    rows = base_ref.shape[0]
    hidden = base_ref[...] + r2_ref[...].astype(F32)
    hid_ref[...] = hidden
    ms = jnp.mean(hidden * hidden, axis=-1, keepdims=True)
    normed = (hidden * lax.rsqrt(ms + norm_eps) * gain_ref[...]).astype(BF16)

    def pick(first, count):
        slot = first + lax.broadcasted_iota(jnp.int32, (count, rows), 0)
        hit = slot == slot_ref[0:1, :]
        for j in range(1, slot_ref.shape[0]):
            hit = hit | (slot == slot_ref[j : j + 1, :])
        return jnp.dot(hit.astype(BF16), normed, preferred_element_type=F32).astype(BF16)

    if cap % 16 == 0:
        picked = pick(0, cap * len(outs))
        for k, ref in enumerate(outs):
            ref[...] = picked[k * cap : (k + 1) * cap, :]
    else:
        for k, ref in enumerate(outs):
            ref[...] = pick(k * cap, cap)


def join_kernel(*refs):
    parts, out_ref = refs[:-1], refs[-1]
    out_ref[...] = jnp.concatenate([r[...] for r in parts], axis=0)


def expert_kernel(nrow, fc, *refs):
    x_refs = refs[:nrow]
    g_ref, u_ref, d_ref, keep_ref, send_ref = refs[nrow:]
    x = jnp.concatenate([r[...] for r in x_refs], axis=0)
    acts = []
    for f in range(g_ref.shape[2] // fc):
        cols = slice(f * fc, (f + 1) * fc)
        gate = jnp.dot(x, g_ref[0, :, cols], preferred_element_type=F32)
        up = jnp.dot(x, u_ref[0, :, cols], preferred_element_type=F32)
        acts.append((gate / (1.0 + jnp.exp(-gate)) * up).astype(BF16))
    act = jnp.concatenate(acts, axis=1)
    half = act.shape[0] // 2
    send_ref[...] = jnp.dot(act[half:], d_ref[0], preferred_element_type=F32).astype(BF16)
    keep_ref[...] = jnp.dot(act[:half], d_ref[0], preferred_element_type=F32).astype(BF16)


def settle_kernel(keep_ref, r1_ref, r2_ref, *outs):
    rows = r2_ref.shape[0]
    each = rows // len(outs)
    total = (
        keep_ref[:rows, :].astype(F32) + r1_ref[:rows, :].astype(F32) + r2_ref[...].astype(F32)
    ).astype(BF16)
    for k, ref in enumerate(outs):
        ref[...] = total[k * each : (k + 1) * each, :]


def combine_kernel(slot_ref, weight_ref, hid_ref, *refs):
    parts, out_ref, w_scr, sem = refs[:-3], refs[-3], refs[-2], refs[-1]
    copies = fetch(((weight_ref, w_scr),), sem)
    back = jnp.concatenate([r[...] for r in parts], axis=0)
    rows = hid_ref.shape[0]
    slot = lax.broadcasted_iota(jnp.int32, (back.shape[0], rows), 0)
    same = lax.broadcasted_iota(jnp.int32, (rows, rows), 0) == lax.broadcasted_iota(
        jnp.int32, (rows, rows), 1
    )
    copies[0].wait()
    total = hid_ref[...]
    for j in range(slot_ref.shape[0]):
        hit = (slot == slot_ref[j : j + 1, :]).astype(BF16)
        weight = jnp.sum(jnp.where(same, w_scr[j : j + 1, :], 0.0), axis=1, keepdims=True)
        total += weight * lax.dot_general(
            hit, back, (((0,), (0,)), ((), ())), preferred_element_type=F32
        )
    out_ref[...] = total.astype(out_ref.dtype)


def shaped(shape, dtype):
    return jax.ShapeDtypeStruct(shape, dtype)


def on_device(
    queries, keys, values, query_gain, key_norm_gain, out_weight, residual, norm_gain,
    expert_gate, expert_up, expert_down, routes, route_weight,
):
    sp_size, tp_size = lax.axis_size("sp"), lax.axis_size("tp")
    sp, tp = lax.axis_index("sp"), lax.axis_index("tp")
    rows = queries.shape[0]
    qw, kw = queries.shape[1], keys.shape[1]
    heads = qw // HEAD_SIZE
    own, width = residual.shape
    route_top = routes.shape[1]
    experts = sp_size * expert_gate.shape[0]
    cap = 2 * max(1, route_top * rows // (tp_size * experts))
    sp1, tp1 = sp.astype(jnp.int32).reshape(1), tp.astype(jnp.int32).reshape(1)

    kv, cosine, sine = pl.pallas_call(
        key_kernel,
        out_shape=(
            shaped((rows, 2 * kw), BF16),
            shaped((rows, HEAD_SIZE), F32),
            shaped((rows, HEAD_SIZE), F32),
        ),
        in_specs=[SM, ANY, ANY, ANY],
        out_specs=(VM, VM, VM),
        scratch_shapes=[
            pltpu.VMEM((rows, kw), BF16),
            pltpu.VMEM((1, HEAD_SIZE), F32),
            pltpu.SemaphoreType.DMA((3,)),
        ],
        compiler_params=params(4),
        name="key_prep",
    )(sp1, key_norm_gain.reshape(1, -1), keys, values)

    half = sp_size // 2
    far = swap(kv, "sp", half)
    near = [swap(kv, "sp", k) for k in range(1, half)]
    far_rest = [swap(far, "sp", k) for k in range(1, half)]
    pieces = [kv] + near + [far] + far_rest
    if len(pieces) > 8:
        each = len(pieces) // 8
        pieces = [jnp.concatenate(pieces[i * each : (i + 1) * each], axis=0) for i in range(8)]

    keys_all = sum(p.shape[0] for p in pieces)
    keep, send = pl.pallas_call(
        lambda *a: attention_kernel(len(pieces), tp_size, *a),
        out_shape=(shaped((rows // 2, width), F32), shaped((rows // 2, width), BF16)),
        in_specs=[SM, VM, VM, ANY, ANY, VM] + [VM] * len(pieces),
        out_specs=(VM, VM),
        scratch_shapes=[
            pltpu.VMEM((rows, keys_all), F32),
            pltpu.VMEM((rows, qw), BF16),
            pltpu.VMEM((rows, qw), BF16),
            pltpu.VMEM((1, HEAD_SIZE), F32),
            pltpu.SemaphoreType.DMA((2,)),
        ],
        compiler_params=params(16),
        name="attend",
    )(tp1, cosine, sine, query_gain.reshape(1, -1), queries, out_weight, *pieces)

    def add_pair(kept, got):
        n = kept.shape[0] // 2
        return pl.pallas_call(
            pair_kernel,
            out_shape=shaped((n, width), BF16),
            in_specs=[VM] * 2,
            out_specs=VM,
            compiler_params=params(4),
            name="add_pair",
        )(kept, got)

    r1 = swap(send, "tp", 1)
    pair = add_pair(keep, r1)
    r2 = swap(pair, "tp", 2)
    slot, base, gain = pl.pallas_call(
        lambda *a: base_kernel(experts, cap, *a),
        out_shape=(
            shaped((route_top, own), jnp.int32),
            shaped((own, width), F32),
            shaped((1, width), F32),
        ),
        in_specs=[SM, ANY, ANY, ANY, ANY, VM, VM],
        out_specs=(VM, VM, VM),
        scratch_shapes=[
            pltpu.VMEM((route_top, own), jnp.int32),
            pltpu.VMEM((own, width), BF16),
            pltpu.SemaphoreType.DMA((3,)),
        ],
        compiler_params=params(4),
        name="base",
    )(sp1, pair, routes.T, residual, norm_gain.reshape(1, -1), keep, r1)

    picked = pl.pallas_call(
        lambda *a: dispatch_kernel(cap, *a),
        out_shape=[shaped((own, width), F32)] + [shaped((cap, width), BF16)] * sp_size,
        in_specs=[VM] * 4,
        out_specs=[VM] * (1 + sp_size),
        compiler_params=params(4),
        name="dispatch",
    )(slot, gain, base, r2)
    hidden, mail = picked[0], picked[1:]

    inbox = [mail[0]] + [swap(mail[k], "sp", k) for k in range(1, sp_size)]
    fe = expert_gate.shape[2]
    fc = 256 if fe % 256 == 0 else fe
    returned = []
    for c in range(2):
        parts = inbox[c * half : (c + 1) * half]
        n = cap * half
        mine = pl.pallas_call(
            join_kernel,
            out_shape=shaped((n, width), BF16),
            in_specs=[VM] * half,
            out_specs=VM,
            compiler_params=params(4),
            name="join",
        )(*parts)
        core = swap(mine, "tp", 1)
        cross = swap(mine, "tp", 2)
        both = swap(cross, "tp", 1)
        keep_e, send_e = pl.pallas_call(
            lambda *a: expert_kernel(4, fc, *a),
            out_shape=(shaped((2 * n, width), BF16), shaped((2 * n, width), BF16)),
            in_specs=[VM] * 7,
            out_specs=(VM, VM),
            compiler_params=params(24),
            name="experts",
        )(mine, cross, core, both, expert_gate, expert_up, expert_down)
        e1 = swap(send_e, "tp", 1)
        e2 = swap(add_pair(keep_e, e1), "tp", 2)
        settled = pl.pallas_call(
            settle_kernel,
            out_shape=[shaped((cap, width), BF16)] * half,
            in_specs=[VM] * 3,
            out_specs=[VM] * half,
            compiler_params=params(4),
            name="settle",
        )(keep_e, e1, e2)
        for k in range(half):
            peer = c * half + k
            returned.append(swap(settled[k], "sp", peer) if peer else settled[k])

    return pl.pallas_call(
        combine_kernel,
        out_shape=shaped((own, width), BF16),
        in_specs=[VM, ANY] + [VM] * (1 + sp_size),
        out_specs=VM,
        scratch_shapes=[pltpu.VMEM((route_top, own), F32), pltpu.SemaphoreType.DMA((1,))],
        compiler_params=params(4),
        name="combine",
    )(slot, route_weight.T, hidden, *returned)


def solution(mesh):
    placed = (
        P("sp", "tp"),
        P("sp", "tp"),
        P("sp", "tp"),
        P(),
        P(),
        P("tp", None),
        P(("sp", "tp"), None),
        P(),
        P("sp", None, "tp"),
        P("sp", None, "tp"),
        P("sp", "tp", None),
        P(("sp", "tp"), None),
        P(("sp", "tp"), None),
    )
    return jax.shard_map(
        on_device, mesh=mesh, in_specs=placed, out_specs=P(("sp", "tp"), None), check_vma=False
    )
```

```python
import functools
import math

import jax
import jax.numpy as jnp
from jax import lax
from jax.experimental import pallas as pl
from jax.experimental.pallas import tpu as pltpu
from jax.sharding import PartitionSpec as P


HEAD_SIZE = 128
GRID_W = 64
norm_eps = 1e-06
theta_base = 10000.0


F32 = jnp.float32
BF16 = jnp.bfloat16
VM = pl.BlockSpec(memory_space=pltpu.VMEM)
SM = pl.BlockSpec(memory_space=pltpu.SMEM)
HBM = pl.BlockSpec(memory_space=pltpu.MemorySpace.HBM)


def params(mib):
    return pltpu.CompilerParams(vmem_limit_bytes=mib * 1024 * 1024)


def swap(x, axis, k):
    n = lax.axis_size(axis)
    return lax.ppermute(x, axis, [(i, i ^ k) for i in range(n)])


def call(kernel, operands, ins, outs, shapes, scratch=(), mib=4):
    operands = [
        pltpu.with_memory_space_constraint(x, pltpu.MemorySpace.HBM) if spec is HBM else x
        for x, spec in zip(operands, ins)
    ]
    return pl.pallas_call(
        kernel,
        out_shape=shapes,
        in_specs=ins,
        out_specs=outs,
        scratch_shapes=list(scratch),
        compiler_params=params(mib),
    )(*operands)


def rotate_norm(x, gain, cosine, sine):
    ms = jnp.mean(x * x, axis=-1, keepdims=True)
    v = x * lax.rsqrt(ms + norm_eps) * gain
    lane = lax.broadcasted_iota(jnp.int32, v.shape, 1)
    quarter = HEAD_SIZE // 4
    turned = jnp.where(
        (lane & (2 * quarter - 1)) < quarter,
        -pltpu.roll(v, HEAD_SIZE - quarter, 1),
        pltpu.roll(v, quarter, 1),
    )
    return v * cosine + turned * sine


def fetch(pairs, sem):
    copies = [pltpu.make_async_copy(src, dst, sem.at[i]) for i, (src, dst) in enumerate(pairs)]
    for c in copies:
        c.start()
    return copies


def key_kernel(sp_ref, gain_ref, k_ref, v_ref, kv_ref, cos_ref, sin_ref, k_scr, g_scr, sem):
    kw = k_scr.shape[1]
    copies = fetch(
        ((k_ref, k_scr), (gain_ref, g_scr), (v_ref, kv_ref.at[:, pl.ds(kw, kw)])), sem
    )
    rows = k_scr.shape[0]
    pos = sp_ref[0] * rows + lax.broadcasted_iota(jnp.int32, (rows, HEAD_SIZE), 0)
    lane = lax.broadcasted_iota(jnp.int32, (rows, HEAD_SIZE), 1)
    shift = GRID_W.bit_length() - 1
    coord = jnp.where(lane < HEAD_SIZE // 2, pos >> shift, pos & (GRID_W - 1)).astype(F32)
    freq = (lane & (HEAD_SIZE // 4 - 1)).astype(F32)
    angles = coord * jnp.exp(freq * (-2.0 * math.log(theta_base) / (HEAD_SIZE // 2)))
    cosine = jnp.cos(angles)
    sine = jnp.sin(angles)
    cos_ref[...] = cosine
    sin_ref[...] = sine
    copies[0].wait()
    copies[1].wait()
    for h in range(kw // HEAD_SIZE):
        cols = slice(h * HEAD_SIZE, (h + 1) * HEAD_SIZE)
        kv_ref[:, cols] = rotate_norm(
            k_scr[:, cols].astype(F32), g_scr[...], cosine, sine
        ).astype(BF16)
    copies[2].wait()


def query_kernel(cos_ref, sin_ref, gain_ref, q_ref, w_ref, out_ref, w_out, q_scr, g_scr, sem):
    copies = fetch(((q_ref, q_scr), (gain_ref, g_scr), (w_ref, w_out)), sem)
    rows = q_scr.shape[0]
    copies[0].wait()
    copies[1].wait()
    for h in range(q_scr.shape[1] // HEAD_SIZE):
        out_ref[h * rows : (h + 1) * rows, :] = rotate_norm(
            q_scr[:, h * HEAD_SIZE : (h + 1) * HEAD_SIZE].astype(F32),
            g_scr[...],
            cos_ref[...],
            sin_ref[...],
        ).astype(BF16)
    copies[2].wait()


def attention_kernel(npieces, tp_size, tp_ref, q_ref, w_ref, *rest):
    kv_refs = rest[:npieces]
    keep_ref, send_ref, s_scr, att_scr = rest[npieces:]
    kw = kv_refs[0].shape[1] // 2
    key_heads = kw // HEAD_SIZE
    rows = att_scr.shape[0]
    heads = q_ref.shape[0] // rows
    members = heads // key_heads
    piece = kv_refs[0].shape[0]
    scale = math.log2(math.e) / math.sqrt(HEAD_SIZE)
    pair = 2 if npieces % 2 == 0 else 1
    span = pair * piece

    def load(i, col):
        return jnp.concatenate(
            [kv_refs[i * pair + j][:, col : col + HEAD_SIZE] for j in range(pair)], axis=0
        )

    for h in range(heads):
        kc = (h // members) * HEAD_SIZE
        q = q_ref[h * rows : (h + 1) * rows, :]
        top = None
        for i in range(npieces // pair):
            s = lax.dot_general(
                q, load(i, kc), (((1,), (1,)), ((), ())), preferred_element_type=F32
            )
            s_scr[:, i * span : (i + 1) * span] = s
            top = s if top is None else jnp.maximum(top, s)
        m = jnp.max(top, axis=-1, keepdims=True) * scale
        total = None
        acc = None
        for i in range(npieces // pair):
            p = jnp.exp2(s_scr[:, i * span : (i + 1) * span] * scale - m)
            total = p if total is None else total + p
            o = jnp.dot(p.astype(BF16), load(i, kw + kc), preferred_element_type=F32)
            acc = o if acc is None else acc + o
        norm = jnp.sum(total, axis=-1, keepdims=True)
        att_scr[:, h * HEAD_SIZE : (h + 1) * HEAD_SIZE] = (acc / norm).astype(BF16)
    t = tp_ref[0]
    block = rows // tp_size
    for half, ref in ((0, keep_ref), (1, send_ref)):
        lhs = jnp.concatenate(
            [
                att_scr[pl.ds(pl.multiple_of((t ^ j) * block, block), block), :]
                for j in range(half, tp_size, 2)
            ],
            axis=0,
        )
        ref[...] = jnp.dot(lhs, w_ref[...], preferred_element_type=F32).astype(ref.dtype)


def pair_kernel(keep_ref, got_ref, *outs):
    first = keep_ref.shape[0] // 2
    for ref in outs:
        here = pl.ds(first, ref.shape[0])
        ref[...] = (keep_ref[here, :].astype(F32) + got_ref[here, :].astype(F32)).astype(ref.dtype)
        first += ref.shape[0]


def base_kernel(
    experts, cap, sp_ref, dep_ref, routes_ref, res_ref, gain_ref, mix_ref, down_ref, keep_ref,
    r1_ref, slot_ref, base_ref, gain_out, mix_out, down_out, routes_scr, res_scr, sem,
):
    copies = fetch(
        (
            (routes_ref, routes_scr),
            (res_ref, res_scr),
            (gain_ref, gain_out),
            (mix_ref, mix_out),
            (down_ref, down_out),
        ),
        sem,
    )
    top, rows = slot_ref.shape
    expert = lax.broadcasted_iota(jnp.int32, (experts, rows), 0)
    before = lax.broadcasted_iota(jnp.int32, (rows, rows), 0) < lax.broadcasted_iota(
        jnp.int32, (rows, rows), 1
    )
    copies[0].wait()
    marks = [(expert == routes_scr[j : j + 1, :]).astype(F32) for j in range(top)]
    earlier = jnp.dot(
        sum(marks).astype(BF16), before.astype(BF16), preferred_element_type=F32
    )
    for j in range(top):
        rank = jnp.sum(earlier * marks[j], axis=0, keepdims=True).astype(jnp.int32)
        slot_ref[j : j + 1, :] = (routes_scr[j : j + 1, :] ^ sp_ref[0]) * cap + rank
    copies[1].wait()
    base_ref[...] = (
        res_scr[...].astype(F32) + keep_ref[:rows, :].astype(F32) + r1_ref[:rows, :].astype(F32)
    )
    for c in copies[2:]:
        c.wait()


def dispatch_kernel(cap, slot_ref, gain_ref, base_ref, r2_ref, hid_ref, *outs):
    rows = base_ref.shape[0]
    hidden = base_ref[...] + r2_ref[...].astype(F32)
    hid_ref[...] = hidden
    ms = jnp.mean(hidden * hidden, axis=-1, keepdims=True)
    normed = (hidden * lax.rsqrt(ms + norm_eps) * gain_ref[...]).astype(BF16)

    def pick(first, count):
        slot = first + lax.broadcasted_iota(jnp.int32, (count, rows), 0)
        hit = slot == slot_ref[0:1, :]
        for j in range(1, slot_ref.shape[0]):
            hit = hit | (slot == slot_ref[j : j + 1, :])
        return jnp.dot(hit.astype(BF16), normed, preferred_element_type=F32).astype(BF16)

    if cap % 16 == 0:
        picked = pick(0, cap * len(outs))
        for k, ref in enumerate(outs):
            ref[...] = picked[k * cap : (k + 1) * cap, :]
    else:
        for k, ref in enumerate(outs):
            ref[...] = pick(k * cap, cap)


def join_kernel(*refs):
    parts, out_ref = refs[:-1], refs[-1]
    out_ref[...] = jnp.concatenate([r[...] for r in parts], axis=0)


def expert_kernel(nrow, fc, *refs):
    x_refs = refs[:nrow]
    g_ref, u_ref, d_ref, keep_ref, send_ref = refs[nrow:]
    x = jnp.concatenate([r[...] for r in x_refs], axis=0)
    acts = []
    for f in range(g_ref.shape[2] // fc):
        cols = slice(f * fc, (f + 1) * fc)
        gate = jnp.dot(x, g_ref[0, :, cols], preferred_element_type=F32)
        up = jnp.dot(x, u_ref[0, :, cols], preferred_element_type=F32)
        acts.append((gate / (1.0 + jnp.exp(-gate)) * up).astype(BF16))
    act = jnp.concatenate(acts, axis=1)
    half = act.shape[0] // 2
    send_ref[...] = jnp.dot(act[half:], d_ref[0], preferred_element_type=F32).astype(BF16)
    keep_ref[...] = jnp.dot(act[:half], d_ref[0], preferred_element_type=F32).astype(BF16)


def settle_kernel(first, keep_ref, r1_ref, r2_ref, *outs):
    rows = r2_ref.shape[0]
    each = rows // len(outs)
    here = pl.ds(first, rows)
    total = (
        keep_ref[here, :].astype(F32) + r1_ref[here, :].astype(F32) + r2_ref[...].astype(F32)
    ).astype(BF16)
    for k, ref in enumerate(outs):
        ref[...] = total[k * each : (k + 1) * each, :]


def combine_kernel(slot_ref, weight_ref, hid_ref, *refs):
    parts, out_ref = refs[:-1], refs[-1]
    back = jnp.concatenate([r[...] for r in parts], axis=0)
    rows = hid_ref.shape[0]
    slot = lax.broadcasted_iota(jnp.int32, (back.shape[0], rows), 0)
    same = lax.broadcasted_iota(jnp.int32, (rows, rows), 0) == lax.broadcasted_iota(
        jnp.int32, (rows, rows), 1
    )
    total = hid_ref[...]
    for j in range(slot_ref.shape[0]):
        hit = (slot == slot_ref[j : j + 1, :]).astype(BF16)
        weight = jnp.sum(jnp.where(same, weight_ref[j : j + 1, :], 0.0), axis=1, keepdims=True)
        total += weight * lax.dot_general(
            hit, back, (((0,), (0,)), ((), ())), preferred_element_type=F32
        )
    out_ref[...] = total.astype(out_ref.dtype)


def shaped(shape, dtype):
    return jax.ShapeDtypeStruct(shape, dtype)


def layer(
    queries, keys, values, query_gain, key_norm_gain, out_weight, residual, norm_gain,
    expert_gate, expert_up, expert_down, routes, route_weight,
):
    sp_size, tp_size = lax.axis_size("sp"), lax.axis_size("tp")
    sp, tp = lax.axis_index("sp"), lax.axis_index("tp")
    rows = queries.shape[0]
    qw, kw = queries.shape[1], keys.shape[1]
    heads = qw // HEAD_SIZE
    own, width = residual.shape
    route_top = routes.shape[1]
    experts = sp_size * expert_gate.shape[0]
    cap = 2 * max(1, route_top * rows // (tp_size * experts))
    sp1, tp1 = sp.astype(jnp.int32).reshape(1), tp.astype(jnp.int32).reshape(1)

    lane = shaped((rows, HEAD_SIZE), F32)
    kv, cosine, sine = call(
        key_kernel,
        (sp1, key_norm_gain.reshape(1, -1), keys, values),
        [SM, HBM, HBM, HBM],
        (VM, VM, VM),
        (shaped((rows, 2 * kw), BF16), lane, lane),
        [
            pltpu.VMEM((rows, kw), BF16),
            pltpu.VMEM((1, HEAD_SIZE), F32),
            pltpu.SemaphoreType.DMA((3,)),
        ],
    )

    half = sp_size // 2
    pieces = [kv] + [swap(kv, "sp", k) for k in range(1, sp_size)]
    if len(pieces) > 8:
        each = len(pieces) // 8
        pieces = [jnp.concatenate(pieces[i * each : (i + 1) * each], axis=0) for i in range(8)]

    q, w_near = call(
        query_kernel,
        (cosine, sine, query_gain.reshape(1, -1), queries, out_weight),
        [VM, VM, HBM, HBM, HBM],
        (VM, VM),
        (shaped((heads * rows, HEAD_SIZE), BF16), shaped(out_weight.shape, BF16)),
        [
            pltpu.VMEM((rows, qw), BF16),
            pltpu.VMEM((1, HEAD_SIZE), F32),
            pltpu.SemaphoreType.DMA((3,)),
        ],
    )

    keys_all = sum(p.shape[0] for p in pieces)
    keep, send = call(
        lambda *a: attention_kernel(len(pieces), tp_size, *a),
        (tp1, q, w_near, *pieces),
        [SM] + [VM] * (2 + len(pieces)),
        (VM, VM),
        (shaped((rows // 2, width), F32), shaped((rows // 2, width), BF16)),
        [pltpu.VMEM((rows, keys_all), F32), pltpu.VMEM((rows, qw), BF16)],
        16,
    )

    def add_pair(kept, got, splits):
        n = kept.shape[0] // (2 * splits)
        return call(
            pair_kernel, (kept, got), [VM] * 2, [VM] * splits, [shaped((n, width), BF16)] * splits
        )

    r1 = swap(send, "tp", 1)
    (pair,) = add_pair(keep, r1, 1)
    r2 = swap(pair, "tp", 2)
    slot, base, gain, mix, down = call(
        lambda *a: base_kernel(experts, cap, *a),
        (
            sp1, pair, routes.T, residual, norm_gain.reshape(1, -1), route_weight.T, expert_down,
            keep, r1,
        ),
        [SM] + [HBM] * 6 + [VM] * 2,
        (VM,) * 5,
        (
            shaped((route_top, own), jnp.int32),
            shaped((own, width), F32),
            shaped((1, width), F32),
            shaped((route_top, own), F32),
            shaped(expert_down.shape, BF16),
        ),
        [
            pltpu.VMEM((route_top, own), jnp.int32),
            pltpu.VMEM((own, width), BF16),
            pltpu.SemaphoreType.DMA((5,)),
        ],
    )

    picked = call(
        lambda *a: dispatch_kernel(cap, *a),
        (slot, gain, base, r2),
        [VM] * 4,
        [VM] * (1 + sp_size),
        [shaped((own, width), F32)] + [shaped((cap, width), BF16)] * sp_size,
    )
    hidden, mail = picked[0], picked[1:]

    inbox = [mail[0]] + [swap(mail[k], "sp", k) for k in range(1, sp_size)]
    fe = expert_gate.shape[2]
    fc = 256 if fe % 256 == 0 else fe
    returned = []
    for c in range(2):
        splits = 2 if c == 1 and half % 2 == 0 else 1
        each = half // splits
        n = cap * each
        mine = [
            call(
                join_kernel,
                inbox[c * half + i * each : c * half + (i + 1) * each],
                [VM] * each,
                VM,
                shaped((n, width), BF16),
            )
            for i in range(splits)
        ]
        core = [swap(m, "tp", 1) for m in mine]
        cross = [swap(m, "tp", 2) for m in mine]
        both = [swap(m, "tp", 1) for m in cross]
        rows_in = mine + cross + core + both
        out = shaped((2 * cap * half, width), BF16)
        keep_e, send_e = call(
            lambda *a: expert_kernel(len(rows_in), fc, *a),
            (*rows_in, expert_gate, expert_up, down),
            [VM] * (len(rows_in) + 3),
            (VM, VM),
            (out, out),
            (),
            24,
        )
        e1 = swap(send_e, "tp", 1)
        pairs = add_pair(keep_e, e1, splits)
        for i, part in enumerate(pairs):
            e2 = swap(part, "tp", 2)
            settled = call(
                functools.partial(settle_kernel, i * n),
                (keep_e, e1, e2),
                [VM] * 3,
                [VM] * each,
                [shaped((cap, width), BF16)] * each,
            )
            for k in range(each):
                peer = c * half + i * each + k
                returned.append(swap(settled[k], "sp", peer) if peer else settled[k])

    return call(
        combine_kernel,
        (slot, mix, hidden, *returned),
        [VM] * (3 + sp_size),
        VM,
        shaped((own, width), BF16),
    )


def solution(mesh):
    placed = (
        P("sp", "tp"),
        P("sp", "tp"),
        P("sp", "tp"),
        P(),
        P(),
        P("tp", None),
        P(("sp", "tp"), None),
        P(),
        P("sp", None, "tp"),
        P("sp", None, "tp"),
        P("sp", "tp", None),
        P(("sp", "tp"), None),
        P(("sp", "tp"), None),
    )
    return jax.shard_map(
        layer, mesh=mesh, in_specs=placed, out_specs=P(("sp", "tp"), None), check_vma=False
    )
```

```python
import functools
import math

import jax
import jax.numpy as jnp
from jax import lax
from jax.experimental import pallas as pl
from jax.experimental.pallas import tpu as pltpu
from jax.sharding import PartitionSpec as P


HEAD_SIZE = 128
GRID_W = 64
norm_eps = 1e-06
theta_base = 10000.0


F32 = jnp.float32
BF16 = jnp.bfloat16
VM = pl.BlockSpec(memory_space=pltpu.VMEM)
SM = pl.BlockSpec(memory_space=pltpu.SMEM)
HBM = pl.BlockSpec(memory_space=pltpu.MemorySpace.HBM)


def params(mib):
    return pltpu.CompilerParams(vmem_limit_bytes=mib * 1024 * 1024)


def swap(x, axis, k):
    n = lax.axis_size(axis)
    return lax.ppermute(x, axis, [(i, i ^ k) for i in range(n)])


def call(kernel, operands, ins, outs, shapes, scratch=(), mib=4):
    operands = [
        pltpu.with_memory_space_constraint(x, pltpu.MemorySpace.HBM) if spec is HBM else x
        for x, spec in zip(operands, ins)
    ]
    return pl.pallas_call(
        kernel,
        out_shape=shapes,
        in_specs=ins,
        out_specs=outs,
        scratch_shapes=list(scratch),
        compiler_params=params(mib),
    )(*operands)


def rotate_norm(x, gain, cosine, sine):
    ms = jnp.mean(x * x, axis=-1, keepdims=True)
    v = x * lax.rsqrt(ms + norm_eps) * gain
    lane = lax.broadcasted_iota(jnp.int32, v.shape, 1)
    quarter = HEAD_SIZE // 4
    turned = jnp.where(
        (lane & (2 * quarter - 1)) < quarter,
        -pltpu.roll(v, HEAD_SIZE - quarter, 1),
        pltpu.roll(v, quarter, 1),
    )
    return v * cosine + turned * sine


def fetch(pairs, sem):
    copies = [pltpu.make_async_copy(src, dst, sem.at[i]) for i, (src, dst) in enumerate(pairs)]
    for c in copies:
        c.start()
    return copies


def key_kernel(sp_ref, gain_ref, k_ref, v_ref, kv_ref, cos_ref, sin_ref, k_scr, g_scr, sem):
    kw = k_scr.shape[1]
    copies = fetch(
        ((k_ref, k_scr), (gain_ref, g_scr), (v_ref, kv_ref.at[:, pl.ds(kw, kw)])), sem
    )
    rows = k_scr.shape[0]
    pos = sp_ref[0] * rows + lax.broadcasted_iota(jnp.int32, (rows, HEAD_SIZE), 0)
    lane = lax.broadcasted_iota(jnp.int32, (rows, HEAD_SIZE), 1)
    shift = GRID_W.bit_length() - 1
    coord = jnp.where(lane < HEAD_SIZE // 2, pos >> shift, pos & (GRID_W - 1)).astype(F32)
    freq = (lane & (HEAD_SIZE // 4 - 1)).astype(F32)
    angles = coord * jnp.exp(freq * (-2.0 * math.log(theta_base) / (HEAD_SIZE // 2)))
    cosine = jnp.cos(angles)
    sine = jnp.sin(angles)
    cos_ref[...] = cosine
    sin_ref[...] = sine
    copies[0].wait()
    copies[1].wait()
    for h in range(kw // HEAD_SIZE):
        cols = slice(h * HEAD_SIZE, (h + 1) * HEAD_SIZE)
        kv_ref[:, cols] = rotate_norm(
            k_scr[:, cols].astype(F32), g_scr[...], cosine, sine
        ).astype(BF16)
    copies[2].wait()


def query_kernel(cos_ref, sin_ref, gain_ref, q_ref, w_ref, out_ref, w_out, q_scr, g_scr, sem):
    copies = fetch(((q_ref, q_scr), (gain_ref, g_scr), (w_ref, w_out)), sem)
    rows = q_scr.shape[0]
    copies[0].wait()
    copies[1].wait()
    for h in range(q_scr.shape[1] // HEAD_SIZE):
        out_ref[h * rows : (h + 1) * rows, :] = rotate_norm(
            q_scr[:, h * HEAD_SIZE : (h + 1) * HEAD_SIZE].astype(F32),
            g_scr[...],
            cos_ref[...],
            sin_ref[...],
        ).astype(BF16)
    copies[2].wait()


def attention_kernel(npieces, tp_size, tp_ref, q_ref, w_ref, *rest):
    kv_refs = rest[:npieces]
    keep_ref, send_ref, s_scr, att_scr = rest[npieces:]
    kw = kv_refs[0].shape[1] // 2
    key_heads = kw // HEAD_SIZE
    rows = att_scr.shape[0]
    heads = q_ref.shape[0] // rows
    members = heads // key_heads
    piece = kv_refs[0].shape[0]
    scale = math.log2(math.e) / math.sqrt(HEAD_SIZE)
    pair = 2 if npieces % 2 == 0 else 1
    span = pair * piece

    def load(i, col):
        return jnp.concatenate(
            [kv_refs[i * pair + j][:, col : col + HEAD_SIZE] for j in range(pair)], axis=0
        )

    for h in range(heads):
        kc = (h // members) * HEAD_SIZE
        q = q_ref[h * rows : (h + 1) * rows, :]
        top = None
        for i in range(npieces // pair):
            s = lax.dot_general(
                q, load(i, kc), (((1,), (1,)), ((), ())), preferred_element_type=F32
            )
            s_scr[:, i * span : (i + 1) * span] = s
            top = s if top is None else jnp.maximum(top, s)
        m = jnp.max(top, axis=-1, keepdims=True) * scale
        total = None
        acc = None
        for i in range(npieces // pair):
            p = jnp.exp2(s_scr[:, i * span : (i + 1) * span] * scale - m)
            total = p if total is None else total + p
            o = jnp.dot(p.astype(BF16), load(i, kw + kc), preferred_element_type=F32)
            acc = o if acc is None else acc + o
        norm = jnp.sum(total, axis=-1, keepdims=True)
        att_scr[:, h * HEAD_SIZE : (h + 1) * HEAD_SIZE] = (acc / norm).astype(BF16)
    t = tp_ref[0]
    block = rows // tp_size
    for half, ref in ((0, keep_ref), (1, send_ref)):
        lhs = jnp.concatenate(
            [
                att_scr[pl.ds(pl.multiple_of((t ^ j) * block, block), block), :]
                for j in range(half, tp_size, 2)
            ],
            axis=0,
        )
        ref[...] = jnp.dot(lhs, w_ref[...], preferred_element_type=F32).astype(ref.dtype)


def pair_kernel(first, keep_ref, got_ref, *outs):
    for ref in outs:
        here = pl.ds(first, ref.shape[0])
        ref[...] = (keep_ref[here, :].astype(F32) + got_ref[here, :].astype(F32)).astype(ref.dtype)
        first += ref.shape[0]


def base_kernel(
    experts, cap, sp_ref, dep_ref, routes_ref, res_ref, gain_ref, mix_ref, down_ref, keep_ref,
    r1_ref, slot_ref, base_ref, gain_out, mix_out, down_out, routes_scr, res_scr, sem,
):
    copies = fetch(
        (
            (routes_ref, routes_scr),
            (res_ref, res_scr),
            (gain_ref, gain_out),
            (mix_ref, mix_out),
            (down_ref, down_out),
        ),
        sem,
    )
    top, rows = slot_ref.shape
    expert = lax.broadcasted_iota(jnp.int32, (experts, rows), 0)
    before = lax.broadcasted_iota(jnp.int32, (rows, rows), 0) < lax.broadcasted_iota(
        jnp.int32, (rows, rows), 1
    )
    copies[0].wait()
    marks = [(expert == routes_scr[j : j + 1, :]).astype(F32) for j in range(top)]
    earlier = jnp.dot(
        sum(marks).astype(BF16), before.astype(BF16), preferred_element_type=F32
    )
    for j in range(top):
        rank = jnp.sum(earlier * marks[j], axis=0, keepdims=True).astype(jnp.int32)
        slot_ref[j : j + 1, :] = (routes_scr[j : j + 1, :] ^ sp_ref[0]) * cap + rank
    copies[1].wait()
    base_ref[...] = (
        res_scr[...].astype(F32) + keep_ref[:rows, :].astype(F32) + r1_ref[:rows, :].astype(F32)
    )
    for c in copies[2:]:
        c.wait()


def dispatch_kernel(cap, slot_ref, gain_ref, base_ref, r2_ref, hid_ref, near_ref, *outs):
    rows = base_ref.shape[0]
    hidden = base_ref[...] + r2_ref[...].astype(F32)
    hid_ref[...] = hidden
    ms = jnp.mean(hidden * hidden, axis=-1, keepdims=True)
    normed = (hidden * lax.rsqrt(ms + norm_eps) * gain_ref[...]).astype(BF16)

    def pick(first, count):
        slot = first + lax.broadcasted_iota(jnp.int32, (count, rows), 0)
        hit = slot == slot_ref[0:1, :]
        for j in range(1, slot_ref.shape[0]):
            hit = hit | (slot == slot_ref[j : j + 1, :])
        return jnp.dot(hit.astype(BF16), normed, preferred_element_type=F32).astype(BF16)

    near = near_ref.shape[0]
    if cap % 16 == 0:
        picked = pick(0, near + cap * len(outs))
        near_ref[...] = picked[:near]
        for k, ref in enumerate(outs):
            ref[...] = picked[near + k * cap : near + (k + 1) * cap, :]
    else:
        near_ref[...] = pick(0, near)
        for k, ref in enumerate(outs):
            ref[...] = pick(near + k * cap, cap)


def fold_kernel(near_ref, got_ref, *outs):
    cap = outs[0].shape[0] // 2
    near, got = near_ref[...], got_ref[...]
    for k, ref in enumerate(outs):
        here = slice(k * cap, (k + 1) * cap)
        ref[...] = jnp.concatenate([near[here], got[here]], axis=0)


def near_pair_kernel(cap, keep_ref, got_ref, *outs):
    first = 0
    for ref in outs:
        for k in range(ref.shape[0] // cap):
            here = pl.ds(first + cap, cap)
            ref[pl.ds(k * cap, cap), :] = (
                keep_ref[here, :].astype(F32) + got_ref[here, :].astype(F32)
            ).astype(BF16)
            first += 2 * cap


def near_settle_kernel(first, keep_ref, r1_ref, r2_ref, *outs):
    for k, ref in enumerate(outs):
        cap = ref.shape[0]
        here = pl.ds(2 * cap * (first + k), cap)
        ref[...] = (
            keep_ref[here, :].astype(F32)
            + r1_ref[here, :].astype(F32)
            + r2_ref[pl.ds(k * cap, cap), :].astype(F32)
        ).astype(BF16)


def join_kernel(*refs):
    parts, out_ref = refs[:-1], refs[-1]
    out_ref[...] = jnp.concatenate([r[...] for r in parts], axis=0)


def expert_kernel(nrow, fc, *refs):
    x_refs = refs[:nrow]
    g_ref, u_ref, d_ref, keep_ref, send_ref = refs[nrow:]
    x = jnp.concatenate([r[...] for r in x_refs], axis=0)
    acts = []
    for f in range(g_ref.shape[2] // fc):
        cols = slice(f * fc, (f + 1) * fc)
        gate = jnp.dot(x, g_ref[0, :, cols], preferred_element_type=F32)
        up = jnp.dot(x, u_ref[0, :, cols], preferred_element_type=F32)
        acts.append((gate / (1.0 + jnp.exp(-gate)) * up).astype(BF16))
    act = jnp.concatenate(acts, axis=1)
    half = act.shape[0] // 2
    send_ref[...] = jnp.dot(act[half:], d_ref[0], preferred_element_type=F32).astype(BF16)
    keep_ref[...] = jnp.dot(act[:half], d_ref[0], preferred_element_type=F32).astype(BF16)


def settle_kernel(first, keep_ref, r1_ref, r2_ref, *outs):
    rows = r2_ref.shape[0]
    each = rows // len(outs)
    here = pl.ds(first, rows)
    total = (
        keep_ref[here, :].astype(F32) + r1_ref[here, :].astype(F32) + r2_ref[...].astype(F32)
    ).astype(BF16)
    for k, ref in enumerate(outs):
        ref[...] = total[k * each : (k + 1) * each, :]


def combine_kernel(slot_ref, weight_ref, hid_ref, *refs):
    parts, out_ref = refs[:-1], refs[-1]
    back = jnp.concatenate([r[...] for r in parts], axis=0)
    rows = hid_ref.shape[0]
    slot = lax.broadcasted_iota(jnp.int32, (back.shape[0], rows), 0)
    same = lax.broadcasted_iota(jnp.int32, (rows, rows), 0) == lax.broadcasted_iota(
        jnp.int32, (rows, rows), 1
    )
    total = hid_ref[...]
    for j in range(slot_ref.shape[0]):
        hit = (slot == slot_ref[j : j + 1, :]).astype(BF16)
        weight = jnp.sum(jnp.where(same, weight_ref[j : j + 1, :], 0.0), axis=1, keepdims=True)
        total += weight * lax.dot_general(
            hit, back, (((0,), (0,)), ((), ())), preferred_element_type=F32
        )
    out_ref[...] = total.astype(out_ref.dtype)


def shaped(shape, dtype):
    return jax.ShapeDtypeStruct(shape, dtype)


def layer(
    queries, keys, values, query_gain, key_norm_gain, out_weight, residual, norm_gain,
    expert_gate, expert_up, expert_down, routes, route_weight,
):
    sp_size, tp_size = lax.axis_size("sp"), lax.axis_size("tp")
    sp, tp = lax.axis_index("sp"), lax.axis_index("tp")
    rows = queries.shape[0]
    qw, kw = queries.shape[1], keys.shape[1]
    heads = qw // HEAD_SIZE
    own, width = residual.shape
    route_top = routes.shape[1]
    experts = sp_size * expert_gate.shape[0]
    cap = 2 * max(1, route_top * rows // (tp_size * experts))
    sp1, tp1 = sp.astype(jnp.int32).reshape(1), tp.astype(jnp.int32).reshape(1)

    lane = shaped((rows, HEAD_SIZE), F32)
    kv, cosine, sine = call(
        key_kernel,
        (sp1, key_norm_gain.reshape(1, -1), keys, values),
        [SM, HBM, HBM, HBM],
        (VM, VM, VM),
        (shaped((rows, 2 * kw), BF16), lane, lane),
        [
            pltpu.VMEM((rows, kw), BF16),
            pltpu.VMEM((1, HEAD_SIZE), F32),
            pltpu.SemaphoreType.DMA((3,)),
        ],
    )

    half = sp_size // 2
    far = swap(kv, "sp", half)
    pieces = [kv] + [swap(kv, "sp", k) for k in range(1, half)]
    pieces += [far] + [swap(far, "sp", k) for k in range(1, half)]
    if len(pieces) > 8:
        each = len(pieces) // 8
        pieces = [jnp.concatenate(pieces[i * each : (i + 1) * each], axis=0) for i in range(8)]

    q, w_near = call(
        query_kernel,
        (cosine, sine, query_gain.reshape(1, -1), queries, out_weight),
        [VM, VM, HBM, HBM, HBM],
        (VM, VM),
        (shaped((heads * rows, HEAD_SIZE), BF16), shaped(out_weight.shape, BF16)),
        [
            pltpu.VMEM((rows, qw), BF16),
            pltpu.VMEM((1, HEAD_SIZE), F32),
            pltpu.SemaphoreType.DMA((3,)),
        ],
    )

    keys_all = sum(p.shape[0] for p in pieces)
    keep, send = call(
        lambda *a: attention_kernel(len(pieces), tp_size, *a),
        (tp1, q, w_near, *pieces),
        [SM] + [VM] * (2 + len(pieces)),
        (VM, VM),
        (shaped((rows // 2, width), F32), shaped((rows // 2, width), BF16)),
        [pltpu.VMEM((rows, keys_all), F32), pltpu.VMEM((rows, qw), BF16)],
        16,
    )

    def add_pair(kept, got, first, splits):
        n = (kept.shape[0] - first) // splits
        return call(
            functools.partial(pair_kernel, first),
            (kept, got),
            [VM] * 2,
            [VM] * splits,
            [shaped((n, width), BF16)] * splits,
        )

    r1 = swap(send, "tp", 1)
    (pair,) = add_pair(keep, r1, own, 1)
    r2 = swap(pair, "tp", 2)
    slot, base, gain, mix, down = call(
        lambda *a: base_kernel(experts, cap, *a),
        (
            sp1, pair, routes.T, residual, norm_gain.reshape(1, -1), route_weight.T, expert_down,
            keep, r1,
        ),
        [SM] + [HBM] * 6 + [VM] * 2,
        (VM,) * 5,
        (
            shaped((route_top, own), jnp.int32),
            shaped((own, width), F32),
            shaped((1, width), F32),
            shaped((route_top, own), F32),
            shaped(expert_down.shape, BF16),
        ),
        [
            pltpu.VMEM((route_top, own), jnp.int32),
            pltpu.VMEM((own, width), BF16),
            pltpu.SemaphoreType.DMA((5,)),
        ],
    )

    near_rows = cap * half
    picked = call(
        lambda *a: dispatch_kernel(cap, *a),
        (slot, gain, base, r2),
        [VM] * 4,
        [VM] * (2 + half),
        [shaped((own, width), F32), shaped((near_rows, width), BF16)]
        + [shaped((cap, width), BF16)] * half,
    )
    hidden, near_block, mail = picked[0], picked[1], picked[2:]
    fe = expert_gate.shape[2]
    fc = 256 if fe % 256 == 0 else fe

    def run(rows_in):
        rows_all = sum(r.shape[0] for r in rows_in)
        out = shaped((rows_all // 2, width), BF16)
        return call(
            lambda *a: expert_kernel(len(rows_in), fc, *a),
            (*rows_in, expert_gate, expert_up, down),
            [VM] * (len(rows_in) + 3),
            (VM, VM),
            (out, out),
            (),
            24,
        )

    def join(parts):
        rows_all = sum(p.shape[0] for p in parts)
        return call(join_kernel, parts, [VM] * len(parts), VM, shaped((rows_all, width), BF16))

    splits = 2 if half % 2 == 0 else 1
    each = half // splits
    inbox = [swap(mail[k], "sp", half + k) for k in range(half)]
    mine = [join(inbox[i * each : (i + 1) * each]) for i in range(splits)]
    core = [swap(m, "tp", 1) for m in mine]
    cross = [swap(m, "tp", 2) for m in mine]
    both = [swap(m, "tp", 1) for m in cross]
    keep_a, send_a = run(mine + core)
    keep_b, send_b = run(cross + both)
    e1a = swap(send_a, "tp", 1)
    e1b = swap(send_b, "tp", 1)
    pairs = add_pair(keep_b, e1b, 0, splits)
    far_back = []
    for i, part in enumerate(pairs):
        e2 = swap(part, "tp", 2)
        settled = call(
            functools.partial(settle_kernel, i * each * cap),
            (keep_a, e1a, e2),
            [VM] * 3,
            [VM] * each,
            [shaped((cap, width), BF16)] * each,
        )
        for k, rows_k in enumerate(settled):
            peer = half + i * each + k
            far_back.append(swap(rows_k, "sp", peer))

    got = swap(near_block, "tp", 2)
    folded = call(
        fold_kernel,
        (near_block, got),
        [VM] * 2,
        [VM] * half,
        [shaped((2 * cap, width), BF16)] * half,
    )
    inbox = [folded[0]] + [swap(folded[k], "sp", k) for k in range(1, half)]
    mine0 = join(inbox)
    core0 = swap(mine0, "tp", 1)
    keep_n, send_n = run([mine0, core0])
    e1 = swap(send_n, "tp", 1)
    pairs = call(
        functools.partial(near_pair_kernel, cap),
        (keep_n, e1),
        [VM] * 2,
        [VM] * splits,
        [shaped((cap * each, width), BF16)] * splits,
    )
    near_back = []
    for i, part in enumerate(pairs):
        e2 = swap(part, "tp", 2)
        settled = call(
            functools.partial(near_settle_kernel, i * each),
            (keep_n, e1, e2),
            [VM] * 3,
            [VM] * each,
            [shaped((cap, width), BF16)] * each,
        )
        for k, rows_k in enumerate(settled):
            peer = i * each + k
            near_back.append(swap(rows_k, "sp", peer) if peer else rows_k)

    return call(
        combine_kernel,
        (slot, mix, hidden, *near_back, *far_back),
        [VM] * (3 + sp_size),
        VM,
        shaped((own, width), BF16),
    )


def solution(mesh):
    placed = (
        P("sp", "tp"),
        P("sp", "tp"),
        P("sp", "tp"),
        P(),
        P(),
        P("tp", None),
        P(("sp", "tp"), None),
        P(),
        P("sp", None, "tp"),
        P("sp", None, "tp"),
        P("sp", "tp", None),
        P(("sp", "tp"), None),
        P(("sp", "tp"), None),
    )
    return jax.shard_map(
        layer, mesh=mesh, in_specs=placed, out_specs=P(("sp", "tp"), None), check_vma=False
    )
```

```python
import functools
import math

import jax
import jax.numpy as jnp
from jax import lax
from jax.experimental import pallas as pl
from jax.experimental.pallas import tpu as pltpu
from jax.sharding import PartitionSpec as P


HEAD_SIZE = 128
GRID_W = 64
norm_eps = 1e-06
theta_base = 10000.0


F32 = jnp.float32
BF16 = jnp.bfloat16
VM = pl.BlockSpec(memory_space=pltpu.VMEM)
SM = pl.BlockSpec(memory_space=pltpu.SMEM)
HBM = pl.BlockSpec(memory_space=pltpu.MemorySpace.HBM)


def params(mib):
    return pltpu.CompilerParams(vmem_limit_bytes=mib * 1024 * 1024)


def swap(x, axis, k):
    n = lax.axis_size(axis)
    return lax.ppermute(x, axis, [(i, i ^ k) for i in range(n)])


def call(kernel, operands, ins, outs, shapes, scratch=(), mib=4):
    operands = [
        pltpu.with_memory_space_constraint(x, pltpu.MemorySpace.HBM) if spec is HBM else x
        for x, spec in zip(operands, ins)
    ]
    return pl.pallas_call(
        kernel,
        out_shape=shapes,
        in_specs=ins,
        out_specs=outs,
        scratch_shapes=list(scratch),
        compiler_params=params(mib),
    )(*operands)


def far_parts(half):
    if half % 4:
        return [half], [half]
    return [half // 2, half // 2], [half // 4, half // 4, half // 2]


def rotate_norm(x, gain, cosine, sine):
    ms = jnp.mean(x * x, axis=-1, keepdims=True)
    v = x * lax.rsqrt(ms + norm_eps) * gain
    lane = lax.broadcasted_iota(jnp.int32, v.shape, 1)
    quarter = HEAD_SIZE // 4
    turned = jnp.where(
        (lane & (2 * quarter - 1)) < quarter,
        -pltpu.roll(v, HEAD_SIZE - quarter, 1),
        pltpu.roll(v, quarter, 1),
    )
    return v * cosine + turned * sine


def fetch(pairs, sem):
    copies = [pltpu.make_async_copy(src, dst, sem.at[i]) for i, (src, dst) in enumerate(pairs)]
    for c in copies:
        c.start()
    return copies


def key_kernel(sp_ref, gain_ref, k_ref, v_ref, kv_ref, cos_ref, sin_ref, k_scr, g_scr, sem):
    kw = k_scr.shape[1]
    copies = fetch(
        ((k_ref, k_scr), (gain_ref, g_scr), (v_ref, kv_ref.at[:, pl.ds(kw, kw)])), sem
    )
    rows = k_scr.shape[0]
    pos = sp_ref[0] * rows + lax.broadcasted_iota(jnp.int32, (rows, HEAD_SIZE), 0)
    lane = lax.broadcasted_iota(jnp.int32, (rows, HEAD_SIZE), 1)
    shift = GRID_W.bit_length() - 1
    coord = jnp.where(lane < HEAD_SIZE // 2, pos >> shift, pos & (GRID_W - 1)).astype(F32)
    freq = (lane & (HEAD_SIZE // 4 - 1)).astype(F32)
    angles = coord * jnp.exp(freq * (-2.0 * math.log(theta_base) / (HEAD_SIZE // 2)))
    cosine = jnp.cos(angles)
    sine = jnp.sin(angles)
    cos_ref[...] = cosine
    sin_ref[...] = sine
    copies[0].wait()
    copies[1].wait()
    for h in range(kw // HEAD_SIZE):
        cols = slice(h * HEAD_SIZE, (h + 1) * HEAD_SIZE)
        kv_ref[:, cols] = rotate_norm(
            k_scr[:, cols].astype(F32), g_scr[...], cosine, sine
        ).astype(BF16)
    copies[2].wait()


def query_kernel(cos_ref, sin_ref, gain_ref, q_ref, w_ref, out_ref, w_out, q_scr, g_scr, sem):
    copies = fetch(((q_ref, q_scr), (gain_ref, g_scr), (w_ref, w_out)), sem)
    rows = q_scr.shape[0]
    copies[0].wait()
    copies[1].wait()
    for h in range(q_scr.shape[1] // HEAD_SIZE):
        out_ref[h * rows : (h + 1) * rows, :] = rotate_norm(
            q_scr[:, h * HEAD_SIZE : (h + 1) * HEAD_SIZE].astype(F32),
            g_scr[...],
            cos_ref[...],
            sin_ref[...],
        ).astype(BF16)
    copies[2].wait()


SCORE_SCALE = math.log2(math.e) / math.sqrt(HEAD_SIZE)


def piece_loader(kv_refs):
    pair = 2 if len(kv_refs) % 2 == 0 else 1

    def load(i, col):
        return jnp.concatenate(
            [kv_refs[i * pair + j][:, col : col + HEAD_SIZE] for j in range(pair)], axis=0
        )

    return load, len(kv_refs) // pair, pair * kv_refs[0].shape[0]


def fold_lanes(x, op):
    parts = [x[:, i : i + HEAD_SIZE] for i in range(0, x.shape[1], HEAD_SIZE)]
    return functools.reduce(op, parts)


def scores_of(q, k):
    return lax.dot_general(q, k, (((1,), (1,)), ((), ())), preferred_element_type=F32)


def attention_start_kernel(npieces, heads, q_ref, *rest):
    kv_refs = rest[:npieces]
    top_ref, sum_ref, acc_ref, s_scr = rest[npieces:]
    load, count, span = piece_loader(kv_refs)
    kw = kv_refs[0].shape[1] // 2
    members = heads // (kw // HEAD_SIZE)
    rows = q_ref.shape[0] // heads
    for h in range(heads):
        kc = (h // members) * HEAD_SIZE
        here = pl.ds(h * rows, rows)
        q = q_ref[here, :]
        top = None
        for i in range(count):
            s = scores_of(q, load(i, kc))
            s_scr[:, i * span : (i + 1) * span] = s
            top = s if top is None else jnp.maximum(top, s)
        top = jnp.max(fold_lanes(top, jnp.maximum), axis=-1, keepdims=True) * SCORE_SCALE
        total = None
        acc = None
        for i in range(count):
            p = jnp.exp2(s_scr[:, i * span : (i + 1) * span] * SCORE_SCALE - top)
            total = p if total is None else total + p
            o = jnp.dot(p.astype(BF16), load(i, kw + kc), preferred_element_type=F32)
            acc = o if acc is None else acc + o
        top_ref[here, :] = jnp.broadcast_to(top, (rows, HEAD_SIZE))
        sum_ref[here, :] = fold_lanes(total, jnp.add)
        acc_ref[here, :] = acc


def attention_kernel(npieces, heads, tp_size, tp_ref, q_ref, w_ref, top_ref, sum_ref, acc_ref, *rest):
    kv_refs = rest[:npieces]
    keep_ref, send_ref, s_scr, att_scr = rest[npieces:]
    load, count, span = piece_loader(kv_refs)
    kw = kv_refs[0].shape[1] // 2
    members = heads // (kw // HEAD_SIZE)
    rows = q_ref.shape[0] // heads
    for h in range(heads):
        kc = (h // members) * HEAD_SIZE
        here = pl.ds(h * rows, rows)
        q = q_ref[here, :]
        top = None
        for i in range(count):
            s = scores_of(q, load(i, kc))
            s_scr[:, i * span : (i + 1) * span] = s
            top = s if top is None else jnp.maximum(top, s)
        top = jnp.max(fold_lanes(top, jnp.maximum), axis=-1, keepdims=True) * SCORE_SCALE
        before = top_ref[here, :]
        top = jnp.maximum(before[:, :1], top)
        shrink = jnp.exp2(before - top)
        total = sum_ref[here, :] * shrink
        acc = acc_ref[here, :] * shrink
        for i in range(count):
            p = jnp.exp2(s_scr[:, i * span : (i + 1) * span] * SCORE_SCALE - top)
            total = total + fold_lanes(p, jnp.add)
            acc = acc + jnp.dot(p.astype(BF16), load(i, kw + kc), preferred_element_type=F32)
        norm = jnp.sum(total, axis=-1, keepdims=True)
        att_scr[:, h * HEAD_SIZE : (h + 1) * HEAD_SIZE] = (acc / norm).astype(BF16)
    t = tp_ref[0]
    block = rows // tp_size
    lhs = jnp.concatenate(
        [
            att_scr[pl.ds(pl.multiple_of((t ^ j) * block, block), block), :]
            for j in [*range(0, tp_size, 2), *range(1, tp_size, 2)]
        ],
        axis=0,
    )
    projected = jnp.dot(lhs, w_ref[...], preferred_element_type=F32)
    keep_ref[...] = projected[: rows // 2].astype(keep_ref.dtype)
    send_ref[...] = projected[rows // 2 :].astype(send_ref.dtype)


def pair_kernel(first, keep_ref, got_ref, *outs):
    for ref in outs:
        here = pl.ds(first, ref.shape[0])
        ref[...] = (keep_ref[here, :].astype(F32) + got_ref[here, :].astype(F32)).astype(ref.dtype)
        first += ref.shape[0]


def base_kernel(
    experts, cap, sp_ref, dep_ref, routes_ref, res_ref, gain_ref, mix_ref, down_ref, keep_ref,
    r1_ref, slot_ref, base_ref, gain_out, mix_out, down_out, routes_scr, res_scr, sem,
):
    copies = fetch(
        (
            (routes_ref, routes_scr),
            (res_ref, res_scr),
            (gain_ref, gain_out),
            (mix_ref, mix_out),
            (down_ref, down_out),
        ),
        sem,
    )
    top, rows = slot_ref.shape
    expert = lax.broadcasted_iota(jnp.int32, (experts, rows), 0)
    before = lax.broadcasted_iota(jnp.int32, (rows, rows), 0) < lax.broadcasted_iota(
        jnp.int32, (rows, rows), 1
    )
    copies[0].wait()
    marks = [(expert == routes_scr[j : j + 1, :]).astype(F32) for j in range(top)]
    earlier = jnp.dot(
        sum(marks).astype(BF16), before.astype(BF16), preferred_element_type=F32
    )
    for j in range(top):
        rank = jnp.sum(earlier * marks[j], axis=0, keepdims=True).astype(jnp.int32)
        slot_ref[j : j + 1, :] = (routes_scr[j : j + 1, :] ^ sp_ref[0]) * cap + rank
    copies[1].wait()
    base_ref[...] = (
        res_scr[...].astype(F32) + keep_ref[:rows, :].astype(F32) + r1_ref[:rows, :].astype(F32)
    )
    for c in copies[2:]:
        c.wait()


def dispatch_kernel(cap, slot_ref, gain_ref, base_ref, r2_ref, hid_ref, near_ref, *outs):
    rows = base_ref.shape[0]
    hidden = base_ref[...] + r2_ref[...].astype(F32)
    hid_ref[...] = hidden
    ms = jnp.mean(hidden * hidden, axis=-1, keepdims=True)
    normed = (hidden * lax.rsqrt(ms + norm_eps) * gain_ref[...]).astype(BF16)

    def pick(first, count):
        slot = first + lax.broadcasted_iota(jnp.int32, (count, rows), 0)
        hit = slot == slot_ref[0:1, :]
        for j in range(1, slot_ref.shape[0]):
            hit = hit | (slot == slot_ref[j : j + 1, :])
        return jnp.dot(hit.astype(BF16), normed, preferred_element_type=F32).astype(BF16)

    near = near_ref.shape[0]
    if cap % 16 == 0:
        picked = pick(0, near + cap * len(outs))
        near_ref[...] = picked[:near]
        for k, ref in enumerate(outs):
            ref[...] = picked[near + k * cap : near + (k + 1) * cap, :]
    else:
        near_ref[...] = pick(0, near)
        for k, ref in enumerate(outs):
            ref[...] = pick(near + k * cap, cap)


def fold_kernel(near_ref, got_ref, *outs):
    cap = outs[0].shape[0] // 2
    near, got = near_ref[...], got_ref[...]
    for k, ref in enumerate(outs):
        here = slice(k * cap, (k + 1) * cap)
        ref[...] = jnp.concatenate([near[here], got[here]], axis=0)


def near_pair_kernel(cap, keep_ref, got_ref, *outs):
    first = 0
    for ref in outs:
        for k in range(ref.shape[0] // cap):
            here = pl.ds(first + cap, cap)
            ref[pl.ds(k * cap, cap), :] = (
                keep_ref[here, :].astype(F32) + got_ref[here, :].astype(F32)
            ).astype(BF16)
            first += 2 * cap


def near_settle_kernel(first, keep_ref, r1_ref, r2_ref, *outs):
    for k, ref in enumerate(outs):
        cap = ref.shape[0]
        here = pl.ds(2 * cap * (first + k), cap)
        ref[...] = (
            keep_ref[here, :].astype(F32)
            + r1_ref[here, :].astype(F32)
            + r2_ref[pl.ds(k * cap, cap), :].astype(F32)
        ).astype(BF16)


def join_kernel(*refs):
    parts, out_ref = refs[:-1], refs[-1]
    out_ref[...] = jnp.concatenate([r[...] for r in parts], axis=0)


def expert_kernel(nrow, fc, *refs):
    x_refs, outs = refs[:nrow], refs[nrow + 3 :]
    g_ref, u_ref, d_ref = refs[nrow : nrow + 3]
    x = jnp.concatenate([r[...] for r in x_refs], axis=0)
    acts = []
    for f in range(g_ref.shape[2] // fc):
        cols = slice(f * fc, (f + 1) * fc)
        gate = jnp.dot(x, g_ref[0, :, cols], preferred_element_type=F32)
        up = jnp.dot(x, u_ref[0, :, cols], preferred_element_type=F32)
        acts.append((gate / (1.0 + jnp.exp(-gate)) * up).astype(BF16))
    act = jnp.concatenate(acts, axis=1)
    down = jnp.dot(act, d_ref[0], preferred_element_type=F32).astype(BF16)
    each = down.shape[0] // len(outs)
    for i, ref in enumerate(outs):
        ref[...] = down[i * each : (i + 1) * each]


def settle_kernel(first, keep_ref, r1_ref, r2_ref, *outs):
    rows = r2_ref.shape[0]
    each = rows // len(outs)
    here = pl.ds(first, rows)
    total = (
        keep_ref[here, :].astype(F32) + r1_ref[here, :].astype(F32) + r2_ref[...].astype(F32)
    ).astype(BF16)
    for k, ref in enumerate(outs):
        ref[...] = total[k * each : (k + 1) * each, :]


def combine_kernel(slot_ref, weight_ref, hid_ref, *refs):
    parts, out_ref = refs[:-1], refs[-1]
    back = jnp.concatenate([r[...] for r in parts], axis=0)
    rows = hid_ref.shape[0]
    slot = lax.broadcasted_iota(jnp.int32, (back.shape[0], rows), 0)
    same = lax.broadcasted_iota(jnp.int32, (rows, rows), 0) == lax.broadcasted_iota(
        jnp.int32, (rows, rows), 1
    )
    total = hid_ref[...]
    for j in range(slot_ref.shape[0]):
        hit = (slot == slot_ref[j : j + 1, :]).astype(BF16)
        weight = jnp.sum(jnp.where(same, weight_ref[j : j + 1, :], 0.0), axis=1, keepdims=True)
        total += weight * lax.dot_general(
            hit, back, (((0,), (0,)), ((), ())), preferred_element_type=F32
        )
    out_ref[...] = total.astype(out_ref.dtype)


def shaped(shape, dtype):
    return jax.ShapeDtypeStruct(shape, dtype)


def layer(
    queries, keys, values, query_gain, key_norm_gain, out_weight, residual, norm_gain,
    expert_gate, expert_up, expert_down, routes, route_weight,
):
    sp_size, tp_size = lax.axis_size("sp"), lax.axis_size("tp")
    sp, tp = lax.axis_index("sp"), lax.axis_index("tp")
    rows = queries.shape[0]
    qw, kw = queries.shape[1], keys.shape[1]
    heads = qw // HEAD_SIZE
    own, width = residual.shape
    route_top = routes.shape[1]
    experts = sp_size * expert_gate.shape[0]
    cap = 2 * max(1, route_top * rows // (tp_size * experts))
    sp1, tp1 = sp.astype(jnp.int32).reshape(1), tp.astype(jnp.int32).reshape(1)

    lane = shaped((rows, HEAD_SIZE), F32)
    kv, cosine, sine = call(
        key_kernel,
        (sp1, key_norm_gain.reshape(1, -1), keys, values),
        [SM, HBM, HBM, HBM],
        (VM, VM, VM),
        (shaped((rows, 2 * kw), BF16), lane, lane),
        [
            pltpu.VMEM((rows, kw), BF16),
            pltpu.VMEM((1, HEAD_SIZE), F32),
            pltpu.SemaphoreType.DMA((3,)),
        ],
    )

    half = sp_size // 2
    far = swap(kv, "sp", half)
    pieces = [kv] + [swap(kv, "sp", k) for k in range(1, half)]
    pieces += [far] + [swap(far, "sp", k) for k in range(1, half)]
    if len(pieces) > 8:
        each = len(pieces) // 8
        pieces = [jnp.concatenate(pieces[i * each : (i + 1) * each], axis=0) for i in range(8)]

    q, w_near = call(
        query_kernel,
        (cosine, sine, query_gain.reshape(1, -1), queries, out_weight),
        [VM, VM, HBM, HBM, HBM],
        (VM, VM),
        (shaped((heads * rows, HEAD_SIZE), BF16), shaped(out_weight.shape, BF16)),
        [
            pltpu.VMEM((rows, qw), BF16),
            pltpu.VMEM((1, HEAD_SIZE), F32),
            pltpu.SemaphoreType.DMA((3,)),
        ],
    )

    cut = len(pieces) - 2 if len(pieces) > 2 else len(pieces) - 1
    early, late = pieces[:cut], pieces[cut:]
    state = call(
        lambda *a: attention_start_kernel(len(early), heads, *a),
        (q, *early),
        [VM] * (1 + len(early)),
        (VM,) * 3,
        (shaped((heads * rows, HEAD_SIZE), F32),) * 3,
        [pltpu.VMEM((rows, sum(p.shape[0] for p in early)), F32)],
        16,
    )
    keep, send = call(
        lambda *a: attention_kernel(len(late), heads, tp_size, *a),
        (tp1, q, w_near, *state, *late),
        [SM] + [VM] * (5 + len(late)),
        (VM, VM),
        (shaped((rows // 2, width), F32), shaped((rows // 2, width), BF16)),
        [
            pltpu.VMEM((rows, sum(p.shape[0] for p in late)), F32),
            pltpu.VMEM((rows, qw), BF16),
        ],
        16,
    )

    def add_pair(kept, got, first, sizes):
        return call(
            functools.partial(pair_kernel, first),
            (kept, got),
            [VM] * 2,
            [VM] * len(sizes),
            [shaped((n, width), BF16) for n in sizes],
        )

    r1 = swap(send, "tp", 1)
    (pair,) = add_pair(keep, r1, own, [own])
    r2 = swap(pair, "tp", 2)
    slot, base, gain, mix, down = call(
        lambda *a: base_kernel(experts, cap, *a),
        (
            sp1, pair, routes.T, residual, norm_gain.reshape(1, -1), route_weight.T, expert_down,
            keep, r1,
        ),
        [SM] + [HBM] * 6 + [VM] * 2,
        (VM,) * 5,
        (
            shaped((route_top, own), jnp.int32),
            shaped((own, width), F32),
            shaped((1, width), F32),
            shaped((route_top, own), F32),
            shaped(expert_down.shape, BF16),
        ),
        [
            pltpu.VMEM((route_top, own), jnp.int32),
            pltpu.VMEM((own, width), BF16),
            pltpu.SemaphoreType.DMA((5,)),
        ],
    )

    near_rows = cap * half
    picked = call(
        lambda *a: dispatch_kernel(cap, *a),
        (slot, gain, base, r2),
        [VM] * 4,
        [VM] * (2 + half),
        [shaped((own, width), F32), shaped((near_rows, width), BF16)]
        + [shaped((cap, width), BF16)] * half,
    )
    hidden, near_block, mail = picked[0], picked[1], picked[2:]
    fe = expert_gate.shape[2]
    fc = 256 if fe % 256 == 0 else fe

    def run(rows_in, blocks):
        rows_all = sum(r.shape[0] for r in rows_in)
        out = shaped((rows_all // blocks, width), BF16)
        return call(
            lambda *a: expert_kernel(len(rows_in), fc, *a),
            (*rows_in, expert_gate, expert_up, down),
            [VM] * (len(rows_in) + 3),
            (VM,) * blocks,
            (out,) * blocks,
            (),
            24,
        )

    def join(parts):
        rows_all = sum(p.shape[0] for p in parts)
        return call(join_kernel, parts, [VM] * len(parts), VM, shaped((rows_all, width), BF16))

    out_sizes, back_sizes = far_parts(half)
    inbox = [swap(mail[k], "sp", half + k) for k in range(half)]
    mine, first = [], 0
    for size in out_sizes:
        mine.append(join(inbox[first : first + size]) if size > 1 else inbox[first])
        first += size
    core = [swap(m, "tp", 1) for m in mine]
    cross = [swap(m, "tp", 2) for m in mine]
    both = [swap(m, "tp", 1) for m in cross]
    keep_a, send_a = run(mine + core, 2)
    keep_b, send_b = run(cross + both, 2)
    e1a = swap(send_a, "tp", 1)
    e1b = swap(send_b, "tp", 1)
    pairs = add_pair(keep_b, e1b, 0, [n * cap for n in back_sizes])
    far_back, first = [], 0
    for part, size in zip(pairs, back_sizes):
        e2 = swap(part, "tp", 2)
        settled = call(
            functools.partial(settle_kernel, first * cap),
            (keep_a, e1a, e2),
            [VM] * 3,
            [VM] * size,
            [shaped((cap, width), BF16)] * size,
        )
        for k, rows_k in enumerate(settled):
            peer = half + first + k
            far_back.append(swap(rows_k, "sp", peer))
        first += size

    got = swap(near_block, "tp", 2)
    folded = call(
        fold_kernel,
        (near_block, got),
        [VM] * 2,
        [VM] * half,
        [shaped((2 * cap, width), BF16)] * half,
    )
    inbox = [folded[0]] + [swap(folded[k], "sp", k) for k in range(1, half)]
    mine0 = join(inbox)
    core0 = swap(mine0, "tp", 1)
    (keep_n,) = run([mine0], 1)
    (send_n,) = run([core0], 1)
    e1 = swap(send_n, "tp", 1)
    splits = 1
    each = half // splits
    pairs = call(
        functools.partial(near_pair_kernel, cap),
        (keep_n, e1),
        [VM] * 2,
        [VM] * splits,
        [shaped((cap * each, width), BF16)] * splits,
    )
    near_back = []
    for i, part in enumerate(pairs):
        e2 = swap(part, "tp", 2)
        settled = call(
            functools.partial(near_settle_kernel, i * each),
            (keep_n, e1, e2),
            [VM] * 3,
            [VM] * each,
            [shaped((cap, width), BF16)] * each,
        )
        for k, rows_k in enumerate(settled):
            peer = i * each + k
            near_back.append(swap(rows_k, "sp", peer) if peer else rows_k)

    return call(
        combine_kernel,
        (slot, mix, hidden, *near_back, *far_back),
        [VM] * (3 + sp_size),
        VM,
        shaped((own, width), BF16),
    )


def solution(mesh):
    placed = (
        P("sp", "tp"),
        P("sp", "tp"),
        P("sp", "tp"),
        P(),
        P(),
        P("tp", None),
        P(("sp", "tp"), None),
        P(),
        P("sp", None, "tp"),
        P("sp", None, "tp"),
        P("sp", "tp", None),
        P(("sp", "tp"), None),
        P(("sp", "tp"), None),
    )
    return jax.shard_map(
        layer, mesh=mesh, in_specs=placed, out_specs=P(("sp", "tp"), None), check_vma=False
    )
```
